32 devices in a mesh: ep: 8 (over z, y), tp: 4 (over x, core).
Axes of the slice: x: 2, y: 2, z: 4, core: 2. Of those that a mesh axis runs over, the one named last changes fastest.
Arguments:
- tokens: bfloat16 [6144, 2048], P('ep', 'tp')
- norm_gain: float32 [2048], P('tp'), may hold values from 0.1 to 1.9
- routing: int32 [6144, 2], P('ep'), may hold values from 0 to 7, as said below
- route_weight: float32 [6144, 2], P('ep'), may hold values from 0.2 to 1
- w_gate: bfloat16 [8, 2048, 512], P('ep', 'tp'), may hold values from -0.125 to 0.125
- w_up: bfloat16 [8, 2048, 512], P('ep', 'tp'), may hold values from -0.125 to 0.125
- w_down: bfloat16 [8, 512, 2048], P('ep', None, 'tp'), may hold values from -0.25 to 0.25
- w_branch_in: bfloat16 [2048, 1024], P('ep', 'tp'), may hold values from -0.125 to 0.125
- w_branch_out: bfloat16 [1024, 2048], P('tp', 'ep'), may hold values from -0.1875 to 0.1875
- branch_gate: float32 [2048], P('tp'), may hold values from -3 to 3
Outputs:
- mixed: bfloat16 [6144, 2048], P('ep', 'tp')
The draws below stay inside these ranges and needn't reach their ends.
Inputs may be any that keep to these rules, and one draw needn't show every extreme that they name: `routing`: each row names two different experts of the same group; expert e belongs to group e // 2. Among the rows of one device (aligned blocks of 768 rows) no expert is named more than 384 times, and in every block all experts of one group are named exactly 384 times.
All inputs are finite; a program needn't handle non-finite values.
Results may differ from the reference program's by a relative error of at most 0.0069.
Values may be sent and summed in bfloat16 or wider, within the bound.
A program may use at most 128 MiB of HBM per device.

```python
import math
import jax
import jax.numpy as jnp
from jax import lax

D = 2048
FF = 512
BR = 1024
GROUPS = 4
TOK_DEV = 768
EXPERTS = 8
CAP = 384
TOKENS = 6144
N_EP = 8
N_TP = 4


def draw_tokens(key, part):
    first, second = jax.random.split(key, 2)
    base = jax.random.normal(first, (TOKENS, D), jnp.float32)
    scales = jnp.exp(jax.random.uniform(second, (N_TP,), jnp.float32, math.log(0.3), math.log(3.0)))
    values = base.reshape(TOKENS, N_TP, D // N_TP) * scales[None, :, None]
    return values.reshape(TOKENS, D).astype(jnp.bfloat16)


def draw_routing(key, part):
    per_group = EXPERTS // GROUPS
    half = TOK_DEV // 2

    def one_block(block):
        block_key = jax.random.fold_in(key, block)
        keys = jax.random.split(block_key, 3 + GROUPS)
        busiest = jax.random.randint(keys[0], (), 0, GROUPS)
        cuts = jax.random.randint(keys[1], (2,), 0, half + 1)
        lower = jnp.min(cuts)
        upper = jnp.max(cuts)
        others = jnp.stack([lower, upper - lower, half - upper])
        group_ids = jnp.arange(GROUPS, dtype=jnp.int32)
        other_place = jnp.clip(group_ids - (group_ids > busiest).astype(jnp.int32), 0, 2)
        counts = jnp.where(group_ids == busiest, half, others[other_place])
        ends = jnp.cumsum(counts)
        starts = ends - counts
        position = jnp.arange(TOK_DEV, dtype=jnp.int32)
        group = jnp.sum((position[:, None] >= ends[None, :]).astype(jnp.int32), axis=1)
        local = position - starts[group]
        orders = jnp.stack([jax.random.permutation(keys[3 + g], per_group) for g in range(GROUPS)]).astype(jnp.int32)
        offset = 1 + local // per_group % (per_group - 1)
        first = orders[group, local % per_group]
        second = orders[group, (local + offset) % per_group]
        paired = jnp.stack([group * per_group + first, group * per_group + second], axis=1)
        shuffle = jax.random.permutation(keys[2], TOK_DEV)
        return paired[shuffle]
    blocks = jax.vmap(one_block)(jnp.arange(N_EP, dtype=jnp.int32))
    return blocks.reshape(TOKENS, 2).astype(jnp.int32)


def levels(rng, shape, cuts, low, high):
    def one(dim, shards_of):
        heights = jax.random.uniform(jax.random.fold_in(jax.random.fold_in(rng, 6), dim), (shards_of,), jnp.float32, low / len(cuts), high / len(cuts))
        return jnp.repeat(jnp.exp(heights), shape[dim] // shards_of).reshape((-1,) + (1,) * (len(shape) - dim - 1))

    gain = one(*cuts[0])
    for cut in cuts[1:]:
        gain = gain * one(*cut)
    return gain


def normal_values(own_key, extent, spread, most, cuts=(), held_as=jnp.bfloat16):
    level = levels(own_key, extent, cuts, -0.22, 0.18) if cuts else 1.0
    array = jax.random.normal(own_key, extent, jnp.float32) * spread * level
    return jnp.minimum(jnp.maximum(array, -most), most).astype(held_as)


def setup_inputs(seed: int = 0) -> dict:
    splits = jax.random.split(jax.random.key(seed), 11)
    return {
        "tokens": draw_tokens(jax.random.fold_in(splits[10], 71), 0),
        "norm_gain": jnp.clip(1.0 + 0.18 * jax.random.normal(splits[1], (D,), jnp.float32), 0.1, 1.9),
        "routing": draw_routing(jax.random.fold_in(splits[10], 71), 0),
        "route_weight": jnp.clip(0.2 + 0.8 * jax.random.uniform(splits[3], (TOKENS, 2), jnp.float32) ** levels(splits[3], (TOKENS, 2), ((0, 8),), -0.2, 0.2), 0.2, 1.0),
        "w_gate": normal_values(splits[4], (EXPERTS, D, FF), D ** -0.5, 0.125, ((0, 8), (1, 4))),
        "w_up": normal_values(splits[5], (EXPERTS, D, FF), D ** -0.5, 0.125, ((0, 8), (1, 4))),
        "w_down": normal_values(splits[6], (EXPERTS, FF, D), FF ** -0.5, 0.25, ((0, 8), (2, 4))),
        "w_branch_in": normal_values(splits[7], (D, BR), D ** -0.5, 0.125, ((0, 8), (1, 4))),
        "w_branch_out": normal_values(splits[8], (BR, D), BR ** -0.5, 0.1875, ((0, 4), (1, 8))),
        "branch_gate": jnp.clip(jax.random.uniform(splits[9], (D,), jnp.float32, -3.0, 3.0) * levels(splits[9], (D,), ((0, 4),), -0.4, 0.0), -3.0, 3.0),
    }


epsilon = 1e-06

def slot_numbers(routing):
    flat_ids = routing.reshape(N_EP, TOK_DEV * 2)
    one_hot = (flat_ids[:, :, None] == jnp.arange(EXPERTS, dtype=jnp.int32)[None, None, :]).astype(jnp.int32)
    before = jnp.cumsum(one_hot, axis=1) - one_hot
    return lax.optimization_barrier(jnp.sum(before * one_hot, axis=2)).reshape(TOKENS, 2).astype(jnp.int32)

def expert(operands):
    inputs, gate_weight, up_weight, down_weight = operands
    gate_sum = jnp.dot(inputs, gate_weight, preferred_element_type=jnp.float32)
    up_sum = jnp.dot(inputs, up_weight, preferred_element_type=jnp.float32)
    hidden = (jax.nn.silu(gate_sum) * up_sum).astype(jnp.bfloat16)
    return jnp.dot(hidden, down_weight, preferred_element_type=jnp.float32).astype(jnp.bfloat16)

def reference(tokens, norm_gain, routing, route_weight, w_gate, w_up, w_down, w_branch_in, w_branch_out, branch_gate):
    floats = tokens.astype(jnp.float32)
    squares = lax.optimization_barrier(jnp.mean(floats * floats, axis=1, keepdims=True))
    normed = (floats * lax.rsqrt(squares + epsilon) * norm_gain).astype(jnp.bfloat16)
    source = (jnp.arange(TOKENS, dtype=jnp.int32) // TOK_DEV)[:, None]
    place = (source * CAP + slot_numbers(routing)).astype(jnp.int32)
    copies = jnp.broadcast_to(normed[:, None, :], (TOKENS, 2, D))
    buffer = jnp.zeros((EXPERTS, N_EP * CAP, D), jnp.bfloat16).at[routing, place].set(copies)
    outputs = lax.map(expert, (buffer, w_gate, w_up, w_down))
    picked = outputs[routing, place].astype(jnp.float32)
    routed = lax.optimization_barrier(jnp.sum(picked * route_weight[:, :, None], axis=1))
    branch_hidden = jax.nn.silu(jnp.dot(normed, w_branch_in, preferred_element_type=jnp.float32)).astype(jnp.bfloat16)
    branch = jnp.dot(branch_hidden, w_branch_out, preferred_element_type=jnp.float32).astype(jnp.bfloat16)
    return (routed + jax.nn.sigmoid(branch_gate) * branch.astype(jnp.float32)).astype(jnp.bfloat16)
```

```python
import functools

import jax
import jax.numpy as jnp
from jax import lax
from jax.experimental import pallas as pl
from jax.experimental.pallas import tpu as pltpu
from jax.sharding import PartitionSpec as P

GROUPS = 4


epsilon = 1e-06


def send_back(result):
    return lax.all_to_all(result, "ep", split_axis=0, concat_axis=0, tiled=True)


def body(
    tokens,
    norm_gain,
    routing,
    route_weight,
    w_gate,
    w_up,
    w_down,
    w_branch_in,
    w_branch_out,
    branch_gate,
):
    token_count, quarter = tokens.shape
    full_width = quarter * lax.axis_size("tp")
    floats = tokens.astype(jnp.float32)
    squares = lax.psum(jnp.sum(floats * floats, axis=1), "tp")
    normed = (floats * lax.rsqrt(squares[:, None] / full_width + epsilon) * norm_gain).astype(
        jnp.bfloat16
    )
    expert_count = lax.axis_size("ep") * w_gate.shape[0]
    capacity = token_count // (expert_count // GROUPS)
    flat_ids = routing.reshape(-1)
    one_hot = (flat_ids[:, None] == jnp.arange(expert_count, dtype=jnp.int32)[None, :]).astype(
        jnp.int32
    )
    before = jnp.cumsum(one_hot, axis=0) - one_hot
    position = flat_ids * capacity + jnp.sum(before * one_hot, axis=1)
    copies = jnp.repeat(normed, 2, axis=0)
    buffer = jnp.zeros((expert_count * capacity, quarter), jnp.bfloat16).at[position].set(copies)
    buffer = buffer.reshape(expert_count, capacity, quarter)
    gate_whole, up_whole, down_whole = (
        lax.all_gather(w_gate[0], "tp", axis=0, tiled=True),
        lax.all_gather(w_up[0], "tp", axis=0, tiled=True),
        lax.all_gather(w_down[0], "tp", axis=1, tiled=True),
    )
    row_split = lax.all_to_all(
        lax.all_to_all(buffer, "ep", split_axis=0, concat_axis=0, tiled=True),
        "tp",
        split_axis=0,
        concat_axis=2,
        tiled=True,
    )
    slot_rows = row_split.reshape(-1, row_split.shape[2])
    gate_sum = jnp.dot(slot_rows, gate_whole, preferred_element_type=jnp.float32)
    up_sum = jnp.dot(slot_rows, up_whole, preferred_element_type=jnp.float32)
    hidden = (jax.nn.silu(gate_sum) * up_sum).astype(jnp.bfloat16)
    result = jnp.dot(hidden, down_whole, preferred_element_type=jnp.float32).astype(jnp.bfloat16)
    feature_split = lax.all_to_all(
        result.reshape(row_split.shape), "tp", split_axis=2, concat_axis=0, tiled=True
    )
    returned = send_back(feature_split)
    picked = returned.reshape(expert_count * capacity, quarter)[position].reshape(
        token_count, 2, quarter
    )
    routed = jnp.sum(picked.astype(jnp.float32) * route_weight[:, :, None], axis=1)
    branch_tokens = lax.all_to_all(normed, "tp", split_axis=0, concat_axis=1, tiled=True)
    in_cols, out_rows = (
        lax.all_gather(w_branch_in, "tp", axis=1, tiled=True),
        lax.all_gather(w_branch_out, "tp", axis=0, tiled=True),
    )
    in_whole, out_whole = (
        lax.all_gather(in_cols, "ep", axis=0, tiled=True),
        lax.all_gather(out_rows, "ep", axis=1, tiled=True),
    )
    branch_hidden = jax.nn.silu(
        jnp.dot(branch_tokens, in_whole, preferred_element_type=jnp.float32)
    ).astype(jnp.bfloat16)
    branch_local = jnp.dot(branch_hidden, out_whole, preferred_element_type=jnp.float32).astype(
        jnp.bfloat16
    )
    branch = lax.all_to_all(branch_local, "tp", split_axis=1, concat_axis=0, tiled=True)
    return (routed + jax.nn.sigmoid(branch_gate) * branch.astype(jnp.float32)).astype(jnp.bfloat16)


BF16, F32 = jnp.bfloat16, jnp.float32
COPIES = 47


def dot(a, b):
    return jnp.dot(a, b, preferred_element_type=F32)


def dot_nt(a, b):
    return lax.dot_general(a, b, (((1,), (1,)), ((), ())), preferred_element_type=F32)


def silu(v):
    return v / (1.0 + jnp.exp(-v))


def pair_kernel(
    tokens,
    gain,
    routing,
    route_weight,
    w_gate,
    w_up,
    w_down,
    w_in,
    w_out,
    branch_gate,
    out,
    gate_y,
    up_y,
    down_y,
    gate_s,
    up_s,
    down_s,
    squares,
    normed,
    in_all,
    out_all,
    slots_out,
    slots,
    slots_s,
    scale_out,
    scale,
    part_out,
    part_own,
    part_in,
    hidden,
    half_out,
    half_own,
    half_in,
    back_out,
    back,
    fold_out,
    fold_own,
    fold_in,
    cross_out,
    cross_in,
    branch_hidden,
    code_col,
    send_sem,
    recv_sem,
):
    ep, tp = lax.axis_index("ep"), lax.axis_index("tp")
    z, y, x, c = ep // 2, ep % 2, tp // 2, tp % 2
    token_count, quarter = tokens.shape
    ff = w_gate.shape[1]
    capacity = slots.shape[1]
    half = capacity // 2
    block = w_in.shape[0]

    def at(zz, yy, xx, cc):
        return (zz * 2 + yy, xx * 2 + cc)

    sibling = at(z, y, x, 1 - c)
    across = at(z, y, 1 - x, c)
    diagonal = at(z, y, 1 - x, 1 - c)
    pair = at(z, 1 - y, x, c)
    ahead = [None] + [at((z + s) % GROUPS, y, x, c) for s in range(1, GROUPS)]
    behind = [None] + [at((z + GROUPS - s) % GROUPS, y, x, c) for s in range(1, GROUPS)]

    barrier = pltpu.get_barrier_semaphore()
    peers = [sibling, across, diagonal, pair] + ahead[1:]
    for peer in peers:
        pl.semaphore_signal(
            barrier, inc=1, device_id=peer, device_id_type=pl.DeviceIdType.MESH
        )
    pl.semaphore_wait(barrier, len(peers))

    started = {}

    def send(number, source, target, device):
        copy = pltpu.make_async_remote_copy(
            src_ref=source,
            dst_ref=target,
            send_sem=send_sem.at[number],
            recv_sem=recv_sem.at[number],
            device_id=device,
            device_id_type=pl.DeviceIdType.MESH,
        )
        copy.start()
        started[number] = copy

    def arrived(number):
        started[number].wait_recv()

    send(0, w_gate, gate_y.at[y], pair)
    send(1, w_up, up_y.at[y], pair)
    send(2, w_down, down_y.at[y], pair)

    floats = tokens[...].astype(F32)
    exact = floats * floats
    high = exact.astype(BF16)
    low = (exact - high.astype(F32)).astype(BF16)
    ones = jnp.ones((16, quarter), BF16)
    squares[0] = (dot_nt(ones, high) + dot_nt(ones, low))[:8]
    send(6, squares.at[0], squares.at[1], sibling)
    send(7, squares.at[0], squares.at[2], across)
    send(8, squares.at[0], squares.at[3], diagonal)

    for s in range(1, GROUPS):
        send(11 + s, w_in, in_all.at[y, z], ahead[s])
        send(14 + s, w_out, out_all.at[y, z], ahead[s])
    in_all[y, z] = w_in[...]
    out_all[y, z] = w_out[...]
    gate_y[y] = w_gate[...]
    up_y[y] = w_up[...]
    down_y[y] = w_down[...]

    ids = routing[0:1, :]
    group = lax.shift_right_logical(ids, 1)
    rows16 = lax.broadcasted_iota(jnp.int32, (16, token_count), 0)
    member = jnp.where(rows16 == group, 1.0, 0.0)
    earlier = jnp.where(
        lax.broadcasted_iota(jnp.int32, (token_count, token_count), 0)
        < lax.broadcasted_iota(jnp.int32, (token_count, token_count), 1),
        1.0,
        0.0,
    ).astype(BF16)
    before = dot(member.astype(BF16), earlier)
    place = jnp.sum(member * before, axis=0, keepdims=True)
    code = group.astype(F32) * capacity + place
    code_col[...] = jnp.transpose(jnp.broadcast_to(code, (8, token_count)))
    first, second = route_weight[0:1, :], route_weight[1:2, :]
    even_first = (ids & 1) == 0
    for_even = jnp.where(even_first, first, second)
    for_odd = jnp.where(even_first, second, first)
    weights = jnp.where((rows16 & 1) == 0, for_even, for_odd)
    weights_high = weights.astype(BF16)
    weights_low = (weights - weights_high.astype(F32)).astype(BF16)

    for number in (6, 7, 8):
        arrived(number)
    total = squares[0] + squares[1] + squares[2] + squares[3]
    factor = lax.rsqrt(total / (4 * quarter) + epsilon)
    factor_col = jnp.transpose(factor)[:, 0:1]
    normed[0] = (tokens[...].astype(F32) * factor_col * gain[...]).astype(BF16)
    send(9, normed.at[0], normed.at[1], sibling)

    slot_row = lax.broadcasted_iota(jnp.int32, (capacity, token_count), 0)
    for s in (2, 1, 3, 0):
        wanted = (slot_row + ((z + s) % GROUPS) * capacity).astype(F32)
        choose = jnp.where(wanted == code, 1.0, 0.0).astype(BF16)
        rows = dot(choose, normed[0]).astype(BF16)
        slot_weights = (dot_nt(weights_high, choose) + dot_nt(weights_low, choose))[:8]
        if s == 0:
            slots[0] = rows
            scale[0] = slot_weights
            send(26, slots.at[0], slots_s.at[0], sibling)
        else:
            slots_out[s] = rows
            scale_out[s] = slot_weights
            send(19 + s, slots_out.at[s], slots.at[s], ahead[s])
            send(22 + s, scale_out.at[s], scale.at[s], ahead[s])
    send(10, normed.at[0], normed.at[2], across)

    def share(number, stage):
        arrived(number)
        whole, rest = stage
        send(number + 3, whole.at[1 - c], rest, sibling)

    def project(s, start):
        own = slots[s, pl.ds(start, half), :]
        other = slots_s[s, pl.ds(start, half), :]
        return (
            dot(own, gate_y[c]) + dot(other, gate_s[...]),
            dot(own, up_y[c]) + dot(other, up_s[...]),
        )

    mine = pl.multiple_of(x * half, half)
    theirs = pl.multiple_of((1 - x) * half, half)

    def forward(s):
        if s:
            arrived(19 + s)
            send(26 + s, slots.at[s], slots_s.at[s], sibling)

    def stage_a(s):
        arrived(26 + s)
        gate_part, up_part = project(s, theirs)
        part_out[s, :, :ff] = gate_part.astype(BF16)
        part_out[s, :, ff:] = up_part.astype(BF16)
        send(30 + s, part_out.at[s], part_in.at[s], across)
        gate_part, up_part = project(s, mine)
        part_own[s, :, :ff] = gate_part
        part_own[s, :, ff:] = up_part

    def stage_b(s):
        arrived(30 + s)
        gate_sum = part_own[s, :, :ff] + part_in[s, :, :ff].astype(F32)
        up_sum = part_own[s, :, ff:] + part_in[s, :, ff:].astype(F32)
        hidden[s, pl.ds(mine, half), :] = (silu(gate_sum) * up_sum).astype(BF16)
        kept = hidden.at[s, pl.ds(mine, half), :]
        send(34 + s, kept, kept, across)

    def stage_c(s):
        arrived(34 + s)
        if s:
            arrived(22 + s)
        columns = jnp.transpose(scale[s])
        weight = jnp.where(c == 0, columns[:, 0:1], columns[:, 1:2])
        units = hidden[s]
        half_out[s] = (dot(units, down_s[...]) * weight).astype(BF16)
        send(38 + s, half_out.at[s], half_in.at[s], sibling)
        half_own[s] = dot(units, down_y[c]) * weight

    def stage_d(s):
        arrived(38 + s)
        both = (half_own[s] + half_in[s].astype(F32)).astype(BF16)
        if s == 0:
            back[0] = both
        else:
            back_out[s] = both
            send(41 + s, back_out.at[s], back.at[s], behind[s])

    share(0, (gate_y, gate_s))
    share(1, (up_y, up_s))
    arrived(3)
    arrived(4)
    stage_a(0)
    forward(1)
    arrived(10)
    send(11, normed.at[2], normed.at[3], sibling)
    stage_a(1)
    share(2, (down_y, down_s))
    for s in range(1, GROUPS):
        arrived(11 + s)
        arrived(14 + s)
    send(18, in_all.at[y], in_all.at[y], pair)
    send(19, out_all.at[y], out_all.at[y], pair)
    stage_b(0)
    order = (0, 1, 3, 2)
    forward(order[2])
    stage_a(order[2])
    stage_b(1)
    arrived(5)
    stage_c(0)
    forward(order[3])
    stage_a(order[3])
    stage_d(0)
    stage_c(1)
    stage_b(order[2])
    stage_d(1)

    arrived(9)
    arrived(11)
    arrived(18)
    quarters = (tp, x * 2 + 1 - c, (1 - x) * 2 + c, (1 - x) * 2 + 1 - c)
    sums = jnp.zeros((token_count, block), F32)
    for k, q in enumerate(quarters):
        sums = sums + dot(normed[k, :, :block], in_all[0, q])
        sums = sums + dot(normed[k, :, block:], in_all[1, q])
    branch_hidden[...] = silu(sums).astype(BF16)
    arrived(19)

    def branch_part(q, side):
        return dot(branch_hidden[...], out_all[side, q])

    for side in range(2):
        columns = slice(side * block, (side + 1) * block)
        fold_out[0, :, columns] = branch_part(quarters[1], side).astype(BF16)
        fold_out[1, :, columns] = branch_part(quarters[3], side).astype(BF16)
    send(45, fold_out, fold_in, sibling)

    stage_c(order[2])
    stage_b(order[3])
    stage_d(order[2])

    arrived(45)
    for side in range(2):
        columns = slice(side * block, (side + 1) * block)
        cross_out[:, columns] = (
            branch_part(quarters[2], side) + fold_in[1, :, columns].astype(F32)
        ).astype(BF16)
    stage_c(order[3])
    send(46, cross_out, cross_in, across)
    stage_d(order[3])
    for side in range(2):
        columns = slice(side * block, (side + 1) * block)
        fold_own[:, columns] = branch_part(quarters[0], side) + fold_in[0, :, columns].astype(F32)

    slot_lane = lax.broadcasted_iota(jnp.int32, (token_count, capacity), 1)

    def restore(s):
        wanted = (slot_lane + ((z + s) % GROUPS) * capacity).astype(F32)
        choose = jnp.where(wanted == code_col[:, 0:1], 1.0, 0.0).astype(BF16)
        return dot(choose, back[s])

    half_own_sum = restore(0)
    for s in (1,) + order[2:]:
        arrived(41 + s)
        half_own_sum = half_own_sum + restore(s)
    arrived(46)
    branch = fold_own[...] + cross_in[...].astype(F32)
    gate = 1.0 / (1.0 + jnp.exp(-branch_gate[...]))
    out[...] = (half_own_sum + gate * branch).astype(BF16)
    for copy in started.values():
        copy.wait_send()


def pair_body(
    tokens,
    norm_gain,
    routing,
    route_weight,
    w_gate,
    w_up,
    w_down,
    w_branch_in,
    w_branch_out,
    branch_gate,
):
    count, quarter = tokens.shape
    ff = w_gate.shape[2]
    block = w_branch_in.shape[0]
    cap = count // 2
    half = cap // 2
    vmem = pltpu.VMEM
    rows = (GROUPS, cap, quarter)
    scratch = [
        vmem((2, quarter, ff), BF16),
        vmem((2, quarter, ff), BF16),
        vmem((2, ff, quarter), BF16),
        vmem((quarter, ff), BF16),
        vmem((quarter, ff), BF16),
        vmem((ff, quarter), BF16),
        vmem((4, 8, count), F32),
        vmem((4, count, quarter), BF16),
        vmem((2, GROUPS, block, block), BF16),
        vmem((2, GROUPS, block, block), BF16),
        vmem(rows, BF16),
        vmem(rows, BF16),
        vmem(rows, BF16),
        vmem((GROUPS, 8, cap), F32),
        vmem((GROUPS, 8, cap), F32),
        vmem((GROUPS, half, 2 * ff), BF16),
        vmem((GROUPS, half, 2 * ff), F32),
        vmem((GROUPS, half, 2 * ff), BF16),
        vmem((GROUPS, cap, ff), BF16),
        vmem(rows, BF16),
        vmem(rows, F32),
        vmem(rows, BF16),
        vmem(rows, BF16),
        vmem(rows, BF16),
        vmem((2, count, quarter), BF16),
        vmem((count, quarter), F32),
        vmem((2, count, quarter), BF16),
        vmem((count, quarter), BF16),
        vmem((count, quarter), BF16),
        vmem((count, block), BF16),
        vmem((count, 8), F32),
        pltpu.SemaphoreType.DMA((COPIES,)),
        pltpu.SemaphoreType.DMA((COPIES,)),
    ]
    return pl.pallas_call(
        pair_kernel,
        out_shape=jax.ShapeDtypeStruct((count, quarter), BF16),
        in_specs=[pl.BlockSpec(memory_space=vmem)] * 10,
        out_specs=pl.BlockSpec(memory_space=vmem),
        scratch_shapes=scratch,
        compiler_params=pltpu.CompilerParams(
            collective_id=0, has_side_effects=True, vmem_limit_bytes=60 * 1024 * 1024
        ),
    )(
        tokens,
        norm_gain[None, :],
        routing.T,
        route_weight.T,
        w_gate[0],
        w_up[0],
        w_down[0],
        w_branch_in,
        w_branch_out,
        branch_gate[None, :],
    )


def solution(mesh):
    return jax.shard_map(
        pair_body if mesh.shape["ep"] == 2 * GROUPS and mesh.shape["tp"] == 4 else body,
        mesh=mesh,
        in_specs=(
            P("ep", "tp"),
            P("tp"),
            P("ep", None),
            P("ep", None),
            P("ep", "tp", None),
            P("ep", "tp", None),
            P("ep", None, "tp"),
            P("ep", "tp"),
            P("tp", "ep"),
            P("tp"),
        ),
        out_specs=P("ep", "tp"),
        check_vma=False,
    )
```

```python
import functools

import jax
import jax.numpy as jnp
from jax import lax
from jax.experimental import pallas as pl
from jax.experimental.pallas import tpu as pltpu
from jax.sharding import PartitionSpec as P

GROUPS = 4


epsilon = 1e-06


def send_back(result):
    return lax.all_to_all(result, "ep", split_axis=0, concat_axis=0, tiled=True)


def body(
    tokens,
    norm_gain,
    routing,
    route_weight,
    w_gate,
    w_up,
    w_down,
    w_branch_in,
    w_branch_out,
    branch_gate,
):
    token_count, quarter = tokens.shape
    full_width = quarter * lax.axis_size("tp")
    floats = tokens.astype(jnp.float32)
    squares = lax.psum(jnp.sum(floats * floats, axis=1), "tp")
    normed = (floats * lax.rsqrt(squares[:, None] / full_width + epsilon) * norm_gain).astype(
        jnp.bfloat16
    )
    expert_count = lax.axis_size("ep") * w_gate.shape[0]
    capacity = token_count // (expert_count // GROUPS)
    flat_ids = routing.reshape(-1)
    one_hot = (flat_ids[:, None] == jnp.arange(expert_count, dtype=jnp.int32)[None, :]).astype(
        jnp.int32
    )
    before = jnp.cumsum(one_hot, axis=0) - one_hot
    position = flat_ids * capacity + jnp.sum(before * one_hot, axis=1)
    copies = jnp.repeat(normed, 2, axis=0)
    buffer = jnp.zeros((expert_count * capacity, quarter), jnp.bfloat16).at[position].set(copies)
    buffer = buffer.reshape(expert_count, capacity, quarter)
    gate_whole, up_whole, down_whole = (
        lax.all_gather(w_gate[0], "tp", axis=0, tiled=True),
        lax.all_gather(w_up[0], "tp", axis=0, tiled=True),
        lax.all_gather(w_down[0], "tp", axis=1, tiled=True),
    )
    row_split = lax.all_to_all(
        lax.all_to_all(buffer, "ep", split_axis=0, concat_axis=0, tiled=True),
        "tp",
        split_axis=0,
        concat_axis=2,
        tiled=True,
    )
    slot_rows = row_split.reshape(-1, row_split.shape[2])
    gate_sum = jnp.dot(slot_rows, gate_whole, preferred_element_type=jnp.float32)
    up_sum = jnp.dot(slot_rows, up_whole, preferred_element_type=jnp.float32)
    hidden = (jax.nn.silu(gate_sum) * up_sum).astype(jnp.bfloat16)
    result = jnp.dot(hidden, down_whole, preferred_element_type=jnp.float32).astype(jnp.bfloat16)
    feature_split = lax.all_to_all(
        result.reshape(row_split.shape), "tp", split_axis=2, concat_axis=0, tiled=True
    )
    returned = send_back(feature_split)
    picked = returned.reshape(expert_count * capacity, quarter)[position].reshape(
        token_count, 2, quarter
    )
    routed = jnp.sum(picked.astype(jnp.float32) * route_weight[:, :, None], axis=1)
    branch_tokens = lax.all_to_all(normed, "tp", split_axis=0, concat_axis=1, tiled=True)
    in_cols, out_rows = (
        lax.all_gather(w_branch_in, "tp", axis=1, tiled=True),
        lax.all_gather(w_branch_out, "tp", axis=0, tiled=True),
    )
    in_whole, out_whole = (
        lax.all_gather(in_cols, "ep", axis=0, tiled=True),
        lax.all_gather(out_rows, "ep", axis=1, tiled=True),
    )
    branch_hidden = jax.nn.silu(
        jnp.dot(branch_tokens, in_whole, preferred_element_type=jnp.float32)
    ).astype(jnp.bfloat16)
    branch_local = jnp.dot(branch_hidden, out_whole, preferred_element_type=jnp.float32).astype(
        jnp.bfloat16
    )
    branch = lax.all_to_all(branch_local, "tp", split_axis=1, concat_axis=0, tiled=True)
    return (routed + jax.nn.sigmoid(branch_gate) * branch.astype(jnp.float32)).astype(jnp.bfloat16)


BF16, F32 = jnp.bfloat16, jnp.float32
COPIES = 53


def dot(a, b):
    return jnp.dot(a, b, preferred_element_type=F32)


def dot_nt(a, b):
    return lax.dot_general(a, b, (((1,), (1,)), ((), ())), preferred_element_type=F32)


def silu(v):
    return v / (1.0 + jnp.exp(-v))


def pair_kernel(
    tokens,
    gain,
    routing,
    route_weight,
    w_gate,
    w_up,
    w_down,
    w_in,
    w_out,
    branch_gate,
    out,
    gate_y,
    up_y,
    down_y,
    gate_s,
    up_s,
    down_s,
    squares,
    normed,
    branch_all,
    slots_out,
    slots,
    slots_s,
    scale_out,
    scale,
    part_out,
    part_own,
    part_in,
    hidden,
    half_out,
    half_own,
    half_in,
    back_out,
    back,
    fold_out,
    fold_own,
    fold_in,
    cross_out,
    cross_in,
    branch_hidden,
    code_col,
    send_sem,
    recv_sem,
):
    ep, tp = lax.axis_index("ep"), lax.axis_index("tp")
    z, y, x, c = ep // 2, ep % 2, tp // 2, tp % 2
    token_count, quarter = tokens.shape
    ff = w_gate.shape[1]
    capacity = slots.shape[1]
    half = capacity // 2
    block = w_in.shape[0]

    def at(zz, yy, xx, cc):
        return (zz * 2 + yy, xx * 2 + cc)

    sibling = at(z, y, x, 1 - c)
    across = at(z, y, 1 - x, c)
    diagonal = at(z, y, 1 - x, 1 - c)
    pair = at(z, 1 - y, x, c)
    level = [z, z + 1 - 2 * (z % 2), (z + 2) % GROUPS, GROUPS - 1 - z]
    peer_of = [None] + [at(level[m], y, x, c) for m in range(1, GROUPS)]
    up = at((z + 1) % GROUPS, y, x, c)
    down = at((z + GROUPS - 1) % GROUPS, y, x, c)

    barrier = pltpu.get_barrier_semaphore()
    peers = [sibling, across, diagonal, pair] + peer_of[1:]
    for peer in peers:
        pl.semaphore_signal(
            barrier, inc=1, device_id=peer, device_id_type=pl.DeviceIdType.MESH
        )

    branch_all[y, z, 0] = w_in[...]
    branch_all[y, z, 1] = w_out[...]
    floats = tokens[...].astype(F32)
    exact = floats * floats
    high = exact.astype(BF16)
    low = (exact - high.astype(F32)).astype(BF16)
    ones = jnp.ones((16, quarter), BF16)
    squares[0] = (dot_nt(ones, high) + dot_nt(ones, low))[:8]

    pl.semaphore_wait(barrier, len(peers))

    started = {}

    def send(number, source, target, device):
        copy = pltpu.make_async_remote_copy(
            src_ref=source,
            dst_ref=target,
            send_sem=send_sem.at[number],
            recv_sem=recv_sem.at[number],
            device_id=device,
            device_id_type=pl.DeviceIdType.MESH,
        )
        copy.start()
        started[number] = copy

    def arrived(number):
        started[number].wait_recv()

    send(6, squares.at[0], squares.at[1], sibling)
    send(7, squares.at[0], squares.at[2], across)
    send(8, squares.at[0], squares.at[3], diagonal)

    send(0, w_gate, gate_y.at[y], pair)
    send(1, w_up, up_y.at[y], pair)
    send(2, w_down, down_y.at[y], pair)

    def relay(hop, upward):
        number = (12 if upward else 47) + hop - 1
        held = z - (hop - 1) if upward else z + (hop - 1)
        came = z - hop if upward else z + hop
        held, came = (held + GROUPS) % GROUPS, (came + GROUPS) % GROUPS
        sends = (z <= GROUPS - 2) & (z >= hop - 1)
        gets = z >= hop
        if not upward:
            sends = (z >= 1) & (z <= GROUPS - hop)
            gets = z <= GROUPS - 1 - hop

        def copy(row):
            return pltpu.make_async_remote_copy(
                src_ref=branch_all.at[y, row],
                dst_ref=branch_all.at[y, row],
                send_sem=send_sem.at[number],
                recv_sem=recv_sem.at[number],
                device_id=up if upward else down,
                device_id_type=pl.DeviceIdType.MESH,
            )

        return sends, gets, lambda: copy(held), lambda: copy(came)

    def relay_start(hop):
        for upward in (True, False):
            sends, _, outgoing, _ = relay(hop, upward)

            @pl.when(sends)
            def _():
                outgoing().start()

    def relay_arrived(hop):
        for upward in (True, False):
            _, gets, _, incoming = relay(hop, upward)

            @pl.when(gets)
            def _():
                incoming().wait_recv()

    def relay_sent(hop):
        for upward in (True, False):
            sends, _, outgoing, _ = relay(hop, upward)

            @pl.when(sends)
            def _():
                outgoing().wait_send()

    relay_start(1)
    gate_y[y] = w_gate[...]
    up_y[y] = w_up[...]
    down_y[y] = w_down[...]

    ids = routing[0:1, :]
    group = lax.shift_right_logical(ids, 1)
    rows16 = lax.broadcasted_iota(jnp.int32, (16, token_count), 0)
    member = jnp.where(rows16 == group, 1.0, 0.0)
    earlier = jnp.where(
        lax.broadcasted_iota(jnp.int32, (token_count, token_count), 0)
        < lax.broadcasted_iota(jnp.int32, (token_count, token_count), 1),
        1.0,
        0.0,
    ).astype(BF16)
    before = dot(member.astype(BF16), earlier)
    place = jnp.sum(member * before, axis=0, keepdims=True)
    code = group.astype(F32) * capacity + place
    code_col[...] = jnp.transpose(jnp.broadcast_to(code, (8, token_count)))
    first, second = route_weight[0:1, :], route_weight[1:2, :]
    even_first = (ids & 1) == 0
    for_even = jnp.where(even_first, first, second)
    for_odd = jnp.where(even_first, second, first)
    weights = jnp.where((rows16 & 1) == 0, for_even, for_odd)
    weights_high = weights.astype(BF16)
    weights_low = (weights - weights_high.astype(F32)).astype(BF16)

    for number in (6, 7, 8):
        arrived(number)
    total = squares[0] + squares[1] + squares[2] + squares[3]
    factor = lax.rsqrt(total / (4 * quarter) + epsilon)
    factor_col = jnp.transpose(factor)[:, 0:1]
    normed[0] = (tokens[...].astype(F32) * factor_col * gain[...]).astype(BF16)
    send(10, normed.at[0], normed.at[2], across)
    send(9, normed.at[0], normed.at[1], sibling)
    relay_arrived(1)
    relay_start(2)

    slot_row = lax.broadcasted_iota(jnp.int32, (capacity, token_count), 0)
    for s in (2, 3, 1, 0):
        wanted = (slot_row + level[s] * capacity).astype(F32)
        choose = jnp.where(wanted == code, 1.0, 0.0).astype(BF16)
        rows = dot(choose, normed[0]).astype(BF16)
        slot_weights = (dot_nt(weights_high, choose) + dot_nt(weights_low, choose))[:8]
        if s == 0:
            slots[0] = rows
            scale[0] = slot_weights
            send(26, slots.at[0], slots_s.at[0], sibling)
        else:
            slots_out[s] = rows
            scale_out[s] = slot_weights
            send(19 + s, slots_out.at[s], slots.at[s], peer_of[s])
            send(22 + s, scale_out.at[s], scale.at[s], peer_of[s])

    def share(number, stage):
        arrived(number)
        whole, rest = stage
        send(number + 3, whole.at[1 - c], rest, sibling)

    def project(s, start):
        own = slots[s, pl.ds(start, half), :]
        other = slots_s[s, pl.ds(start, half), :]
        return (
            dot(own, gate_y[c]) + dot(other, gate_s[...]),
            dot(own, up_y[c]) + dot(other, up_s[...]),
        )

    mine = pl.multiple_of(x * half, half)
    theirs = pl.multiple_of((1 - x) * half, half)

    def forward(s):
        if s:
            arrived(19 + s)
            send(26 + s, slots.at[s], slots_s.at[s], sibling)

    def stage_a(s):
        arrived(26 + s)
        gate_part, up_part = project(s, theirs)
        part_out[s, :, :ff] = gate_part.astype(BF16)
        part_out[s, :, ff:] = up_part.astype(BF16)
        send(30 + s, part_out.at[s], part_in.at[s], across)
        gate_part, up_part = project(s, mine)
        part_own[s, :, :ff] = gate_part
        part_own[s, :, ff:] = up_part

    def stage_b(s):
        arrived(30 + s)
        gate_sum = part_own[s, :, :ff] + part_in[s, :, :ff].astype(F32)
        up_sum = part_own[s, :, ff:] + part_in[s, :, ff:].astype(F32)
        hidden[s, pl.ds(mine, half), :] = (silu(gate_sum) * up_sum).astype(BF16)
        kept = hidden.at[s, pl.ds(mine, half), :]
        send(34 + s, kept, kept, across)

    def stage_c(s):
        arrived(34 + s)
        if s:
            arrived(22 + s)
        columns = jnp.transpose(scale[s])
        weight = jnp.where(c == 0, columns[:, 0:1], columns[:, 1:2])
        units = hidden[s]
        half_out[s] = (dot(units, down_s[...]) * weight).astype(BF16)
        send(38 + s, half_out.at[s], half_in.at[s], sibling)
        half_own[s] = dot(units, down_y[c]) * weight

    def stage_d(s):
        arrived(38 + s)
        both = (half_own[s] + half_in[s].astype(F32)).astype(BF16)
        if s == 0:
            back[0] = both
        else:
            back_out[s] = both
            send(41 + s, back_out.at[s], back.at[s], peer_of[s])

    share(0, (gate_y, gate_s))
    relay_arrived(2)
    relay_start(3)
    forward(2)
    share(1, (up_y, up_s))
    arrived(3)
    arrived(4)
    stage_a(2)
    stage_a(0)
    arrived(10)
    send(11, normed.at[2], normed.at[3], sibling)
    share(2, (down_y, down_s))
    relay_arrived(3)
    send(18, branch_all.at[y], branch_all.at[y], pair)
    stage_b(2)
    forward(3)
    stage_a(3)
    stage_b(0)
    arrived(5)
    stage_c(2)
    stage_d(2)
    forward(1)
    stage_a(1)
    stage_b(3)
    stage_c(0)
    stage_d(0)

    arrived(9)
    arrived(11)
    arrived(18)
    quarters = (tp, x * 2 + 1 - c, (1 - x) * 2 + c, (1 - x) * 2 + 1 - c)
    sums = jnp.zeros((token_count, block), F32)
    for k, q in enumerate(quarters):
        sums = sums + dot(normed[k, :, :block], branch_all[0, q, 0])
        sums = sums + dot(normed[k, :, block:], branch_all[1, q, 0])
    branch_hidden[...] = silu(sums).astype(BF16)

    def branch_part(q, side):
        return dot(branch_hidden[...], branch_all[side, q, 1])

    for side in range(2):
        columns = slice(side * block, (side + 1) * block)
        fold_out[0, :, columns] = branch_part(quarters[1], side).astype(BF16)
        fold_out[1, :, columns] = branch_part(quarters[3], side).astype(BF16)
    send(45, fold_out, fold_in, sibling)

    stage_b(1)
    stage_c(3)
    stage_d(3)

    arrived(45)
    for side in range(2):
        columns = slice(side * block, (side + 1) * block)
        cross_out[:, columns] = (
            branch_part(quarters[2], side) + fold_in[1, :, columns].astype(F32)
        ).astype(BF16)
    send(46, cross_out, cross_in, across)
    stage_c(1)
    stage_d(1)
    for side in range(2):
        columns = slice(side * block, (side + 1) * block)
        fold_own[:, columns] = branch_part(quarters[0], side) + fold_in[0, :, columns].astype(F32)

    slot_lane = lax.broadcasted_iota(jnp.int32, (token_count, capacity), 1)

    def restore(s):
        wanted = (slot_lane + level[s] * capacity).astype(F32)
        choose = jnp.where(wanted == code_col[:, 0:1], 1.0, 0.0).astype(BF16)
        return dot(choose, back[s])

    half_own_sum = restore(0)
    for s in (2, 3, 1):
        arrived(41 + s)
        half_own_sum = half_own_sum + restore(s)
    arrived(46)
    branch = fold_own[...] + cross_in[...].astype(F32)
    gate = 1.0 / (1.0 + jnp.exp(-branch_gate[...]))
    out[...] = (half_own_sum + gate * branch).astype(BF16)
    for copy in started.values():
        copy.wait_send()
    for hop in range(1, GROUPS):
        relay_sent(hop)


def pair_body(
    tokens,
    norm_gain,
    routing,
    route_weight,
    w_gate,
    w_up,
    w_down,
    w_branch_in,
    w_branch_out,
    branch_gate,
):
    count, quarter = tokens.shape
    ff = w_gate.shape[2]
    block = w_branch_in.shape[0]
    cap = count // 2
    half = cap // 2
    vmem = pltpu.VMEM
    rows = (GROUPS, cap, quarter)
    scratch = [
        vmem((2, quarter, ff), BF16),
        vmem((2, quarter, ff), BF16),
        vmem((2, ff, quarter), BF16),
        vmem((quarter, ff), BF16),
        vmem((quarter, ff), BF16),
        vmem((ff, quarter), BF16),
        vmem((4, 8, count), F32),
        vmem((4, count, quarter), BF16),
        vmem((2, GROUPS, 2, block, block), BF16),
        vmem(rows, BF16),
        vmem(rows, BF16),
        vmem(rows, BF16),
        vmem((GROUPS, 8, cap), F32),
        vmem((GROUPS, 8, cap), F32),
        vmem((GROUPS, half, 2 * ff), BF16),
        vmem((GROUPS, half, 2 * ff), F32),
        vmem((GROUPS, half, 2 * ff), BF16),
        vmem((GROUPS, cap, ff), BF16),
        vmem(rows, BF16),
        vmem(rows, F32),
        vmem(rows, BF16),
        vmem(rows, BF16),
        vmem(rows, BF16),
        vmem((2, count, quarter), BF16),
        vmem((count, quarter), F32),
        vmem((2, count, quarter), BF16),
        vmem((count, quarter), BF16),
        vmem((count, quarter), BF16),
        vmem((count, block), BF16),
        vmem((count, 8), F32),
        pltpu.SemaphoreType.DMA((COPIES,)),
        pltpu.SemaphoreType.DMA((COPIES,)),
    ]
    return pl.pallas_call(
        pair_kernel,
        out_shape=jax.ShapeDtypeStruct((count, quarter), BF16),
        in_specs=[pl.BlockSpec(memory_space=vmem)] * 10,
        out_specs=pl.BlockSpec(memory_space=vmem),
        scratch_shapes=scratch,
        compiler_params=pltpu.CompilerParams(
            collective_id=0, has_side_effects=True, vmem_limit_bytes=60 * 1024 * 1024
        ),
    )(
        tokens,
        norm_gain[None, :],
        routing.T,
        route_weight.T,
        w_gate[0],
        w_up[0],
        w_down[0],
        w_branch_in,
        w_branch_out,
        branch_gate[None, :],
    )


def solution(mesh):
    return jax.shard_map(
        pair_body if mesh.shape["ep"] == 2 * GROUPS and mesh.shape["tp"] == 4 else body,
        mesh=mesh,
        in_specs=(
            P("ep", "tp"),
            P("tp"),
            P("ep", None),
            P("ep", None),
            P("ep", "tp", None),
            P("ep", "tp", None),
            P("ep", None, "tp"),
            P("ep", "tp"),
            P("tp", "ep"),
            P("tp"),
        ),
        out_specs=P("ep", "tp"),
        check_vma=False,
    )
```

```python
import functools

import jax
import jax.numpy as jnp
from jax import lax
from jax.experimental import pallas as pl
from jax.experimental.pallas import tpu as pltpu
from jax.sharding import PartitionSpec as P

GROUPS = 4


epsilon = 1e-06


def send_back(result):
    return lax.all_to_all(result, "ep", split_axis=0, concat_axis=0, tiled=True)


def body(
    tokens,
    norm_gain,
    routing,
    route_weight,
    w_gate,
    w_up,
    w_down,
    w_branch_in,
    w_branch_out,
    branch_gate,
):
    token_count, quarter = tokens.shape
    full_width = quarter * lax.axis_size("tp")
    floats = tokens.astype(jnp.float32)
    squares = lax.psum(jnp.sum(floats * floats, axis=1), "tp")
    normed = (floats * lax.rsqrt(squares[:, None] / full_width + epsilon) * norm_gain).astype(
        jnp.bfloat16
    )
    expert_count = lax.axis_size("ep") * w_gate.shape[0]
    capacity = token_count // (expert_count // GROUPS)
    flat_ids = routing.reshape(-1)
    one_hot = (flat_ids[:, None] == jnp.arange(expert_count, dtype=jnp.int32)[None, :]).astype(
        jnp.int32
    )
    before = jnp.cumsum(one_hot, axis=0) - one_hot
    position = flat_ids * capacity + jnp.sum(before * one_hot, axis=1)
    copies = jnp.repeat(normed, 2, axis=0)
    buffer = jnp.zeros((expert_count * capacity, quarter), jnp.bfloat16).at[position].set(copies)
    buffer = buffer.reshape(expert_count, capacity, quarter)
    gate_whole, up_whole, down_whole = (
        lax.all_gather(w_gate[0], "tp", axis=0, tiled=True),
        lax.all_gather(w_up[0], "tp", axis=0, tiled=True),
        lax.all_gather(w_down[0], "tp", axis=1, tiled=True),
    )
    row_split = lax.all_to_all(
        lax.all_to_all(buffer, "ep", split_axis=0, concat_axis=0, tiled=True),
        "tp",
        split_axis=0,
        concat_axis=2,
        tiled=True,
    )
    slot_rows = row_split.reshape(-1, row_split.shape[2])
    gate_sum = jnp.dot(slot_rows, gate_whole, preferred_element_type=jnp.float32)
    up_sum = jnp.dot(slot_rows, up_whole, preferred_element_type=jnp.float32)
    hidden = (jax.nn.silu(gate_sum) * up_sum).astype(jnp.bfloat16)
    result = jnp.dot(hidden, down_whole, preferred_element_type=jnp.float32).astype(jnp.bfloat16)
    feature_split = lax.all_to_all(
        result.reshape(row_split.shape), "tp", split_axis=2, concat_axis=0, tiled=True
    )
    returned = send_back(feature_split)
    picked = returned.reshape(expert_count * capacity, quarter)[position].reshape(
        token_count, 2, quarter
    )
    routed = jnp.sum(picked.astype(jnp.float32) * route_weight[:, :, None], axis=1)
    branch_tokens = lax.all_to_all(normed, "tp", split_axis=0, concat_axis=1, tiled=True)
    in_cols, out_rows = (
        lax.all_gather(w_branch_in, "tp", axis=1, tiled=True),
        lax.all_gather(w_branch_out, "tp", axis=0, tiled=True),
    )
    in_whole, out_whole = (
        lax.all_gather(in_cols, "ep", axis=0, tiled=True),
        lax.all_gather(out_rows, "ep", axis=1, tiled=True),
    )
    branch_hidden = jax.nn.silu(
        jnp.dot(branch_tokens, in_whole, preferred_element_type=jnp.float32)
    ).astype(jnp.bfloat16)
    branch_local = jnp.dot(branch_hidden, out_whole, preferred_element_type=jnp.float32).astype(
        jnp.bfloat16
    )
    branch = lax.all_to_all(branch_local, "tp", split_axis=1, concat_axis=0, tiled=True)
    return (routed + jax.nn.sigmoid(branch_gate) * branch.astype(jnp.float32)).astype(jnp.bfloat16)


BF16, F32 = jnp.bfloat16, jnp.float32
COPIES = 53


def dot(a, b):
    return jnp.dot(a, b, preferred_element_type=F32)


def dot_nt(a, b):
    return lax.dot_general(a, b, (((1,), (1,)), ((), ())), preferred_element_type=F32)


def silu(v):
    return v / (1.0 + jnp.exp(-v))


def pair_kernel(
    tokens,
    gain,
    routing,
    route_weight,
    w_gate,
    w_up,
    w_down,
    w_in,
    w_out,
    branch_gate,
    out,
    gate_all,
    up_all,
    down_all,
    squares,
    normed,
    branch_all,
    slots_out,
    slots,
    slots_s,
    scale_out,
    scale,
    part_out,
    part_own,
    part_in,
    hidden,
    half_out,
    half_own,
    half_in,
    back_out,
    back,
    fold_out,
    fold_own,
    fold_in,
    cross_out,
    cross_in,
    branch_hidden,
    code_col,
    send_sem,
    recv_sem,
):
    ep, tp = lax.axis_index("ep"), lax.axis_index("tp")
    z, y, x, c = ep // 2, ep % 2, tp // 2, tp % 2
    token_count, quarter = tokens.shape
    ff = w_gate.shape[1]
    capacity = slots.shape[1]
    half = capacity // 2
    block = w_in.shape[0]

    def at(zz, yy, xx, cc):
        return (zz * 2 + yy, xx * 2 + cc)

    sibling = at(z, y, x, 1 - c)
    across = at(z, y, 1 - x, c)
    diagonal = at(z, y, 1 - x, 1 - c)
    pair = at(z, 1 - y, x, c)
    pair_user = at(z, 1 - y, x, y)
    pair_other = at(z, 1 - y, x, 1 - c)
    level = [z, z + 1 - 2 * (z % 2), (z + 2) % GROUPS, GROUPS - 1 - z]
    peer_of = [None] + [at(level[m], y, x, c) for m in range(1, GROUPS)]
    up = at((z + 1) % GROUPS, y, x, c)
    down = at((z + GROUPS - 1) % GROUPS, y, x, c)

    barrier = pltpu.get_barrier_semaphore()
    peers = [sibling, across, diagonal, pair, pair_other] + peer_of[1:]
    for peer in peers:
        pl.semaphore_signal(
            barrier, inc=1, device_id=peer, device_id_type=pl.DeviceIdType.MESH
        )

    branch_all[y, z, 0] = w_in[...]
    branch_all[y, z, 1] = w_out[...]
    floats = tokens[...].astype(F32)
    exact = floats * floats
    high = exact.astype(BF16)
    low = (exact - high.astype(F32)).astype(BF16)
    ones = jnp.ones((16, quarter), BF16)
    squares[0] = (dot_nt(ones, high) + dot_nt(ones, low))[:8]

    pl.semaphore_wait(barrier, len(peers))

    started = {}

    def send(number, source, target, device):
        copy = pltpu.make_async_remote_copy(
            src_ref=source,
            dst_ref=target,
            send_sem=send_sem.at[number],
            recv_sem=recv_sem.at[number],
            device_id=device,
            device_id_type=pl.DeviceIdType.MESH,
        )
        copy.start()
        started[number] = copy

    def arrived(number):
        started[number].wait_recv()

    send(6, squares.at[0], squares.at[1], sibling)
    send(7, squares.at[0], squares.at[2], across)
    send(8, squares.at[0], squares.at[3], diagonal)

    weights_of = ((w_gate, gate_all), (w_up, up_all), (w_down, down_all))

    def weight_copy(k, sem, device):
        source, target = weights_of[k]
        return pltpu.make_async_remote_copy(
            src_ref=source,
            dst_ref=target.at[c],
            send_sem=send_sem.at[2 * k + sem],
            recv_sem=recv_sem.at[2 * k + c],
            device_id=device,
            device_id_type=pl.DeviceIdType.MESH,
        )

    for k in range(3):
        weight_copy(k, 0, pair_user).start()

    @pl.when(c != y)
    def _():
        for k in range(3):
            weight_copy(k, 1, sibling).start()

    @pl.when(c == y)
    def _():
        for source, target in weights_of:
            target[c] = source[...]

    def weight_arrived(k):
        source, target = weights_of[k]

        def wait(h):
            pltpu.make_async_remote_copy(
                src_ref=source,
                dst_ref=target.at[h],
                send_sem=send_sem.at[2 * k],
                recv_sem=recv_sem.at[2 * k + h],
                device_id=sibling,
                device_id_type=pl.DeviceIdType.MESH,
            ).wait_recv()

        wait(1 - c)

        @pl.when(c != y)
        def _():
            wait(c)

    def relay(hop, upward):
        number = (12 if upward else 47) + hop - 1
        held = z - (hop - 1) if upward else z + (hop - 1)
        came = z - hop if upward else z + hop
        held, came = (held + GROUPS) % GROUPS, (came + GROUPS) % GROUPS
        sends = (z <= GROUPS - 2) & (z >= hop - 1)
        gets = z >= hop
        if not upward:
            sends = (z >= 1) & (z <= GROUPS - hop)
            gets = z <= GROUPS - 1 - hop

        def copy(row):
            return pltpu.make_async_remote_copy(
                src_ref=branch_all.at[y, row],
                dst_ref=branch_all.at[y, row],
                send_sem=send_sem.at[number],
                recv_sem=recv_sem.at[number],
                device_id=up if upward else down,
                device_id_type=pl.DeviceIdType.MESH,
            )

        return sends, gets, lambda: copy(held), lambda: copy(came)

    def relay_start(hop):
        for upward in (True, False):
            sends, _, outgoing, _ = relay(hop, upward)

            @pl.when(sends)
            def _():
                outgoing().start()

    def relay_arrived(hop):
        for upward in (True, False):
            _, gets, _, incoming = relay(hop, upward)

            @pl.when(gets)
            def _():
                incoming().wait_recv()

    def relay_sent(hop):
        for upward in (True, False):
            sends, _, outgoing, _ = relay(hop, upward)

            @pl.when(sends)
            def _():
                outgoing().wait_send()

    relay_start(1)
    ids = routing[0:1, :]
    group = lax.shift_right_logical(ids, 1)
    rows16 = lax.broadcasted_iota(jnp.int32, (16, token_count), 0)
    member = jnp.where(rows16 == group, 1.0, 0.0)
    earlier = jnp.where(
        lax.broadcasted_iota(jnp.int32, (token_count, token_count), 0)
        < lax.broadcasted_iota(jnp.int32, (token_count, token_count), 1),
        1.0,
        0.0,
    ).astype(BF16)
    before = dot(member.astype(BF16), earlier)
    place = jnp.sum(member * before, axis=0, keepdims=True)
    code = group.astype(F32) * capacity + place
    code_col[...] = jnp.transpose(jnp.broadcast_to(code, (8, token_count)))
    first, second = route_weight[0:1, :], route_weight[1:2, :]
    even_first = (ids & 1) == 0
    for_even = jnp.where(even_first, first, second)
    for_odd = jnp.where(even_first, second, first)
    weights = jnp.where((rows16 & 1) == 0, for_even, for_odd)
    weights_high = weights.astype(BF16)
    weights_low = (weights - weights_high.astype(F32)).astype(BF16)

    for number in (6, 7, 8):
        arrived(number)
    total = squares[0] + squares[1] + squares[2] + squares[3]
    factor = lax.rsqrt(total / (4 * quarter) + epsilon)
    factor_col = jnp.transpose(factor)[:, 0:1]
    normed[0] = (tokens[...].astype(F32) * factor_col * gain[...]).astype(BF16)
    send(10, normed.at[0], normed.at[2], across)
    send(9, normed.at[0], normed.at[1], sibling)
    relay_arrived(1)
    relay_start(2)

    def dispatch(s):
        send(19 + s, slots_out.at[s], slots.at[s], peer_of[s])
        send(22 + s, scale_out.at[s], scale.at[s], peer_of[s])

    slot_row = lax.broadcasted_iota(jnp.int32, (capacity, token_count), 0)
    for s in (2, 3, 1, 0):
        wanted = (slot_row + level[s] * capacity).astype(F32)
        choose = jnp.where(wanted == code, 1.0, 0.0).astype(BF16)
        rows = dot(choose, normed[0]).astype(BF16)
        slot_weights = (dot_nt(weights_high, choose) + dot_nt(weights_low, choose))[:8]
        if s == 0:
            slots[0] = rows
            scale[0] = slot_weights
            send(26, slots.at[0], slots_s.at[0], sibling)
        else:
            slots_out[s] = rows
            scale_out[s] = slot_weights
            if s > 1:
                dispatch(s)

    def project(s, start, weights):
        own = slots[s, pl.ds(start, half), :]
        other = slots_s[s, pl.ds(start, half), :]
        return dot(own, weights[c]) + dot(other, weights[1 - c])

    mine = pl.multiple_of(x * half, half)
    theirs = pl.multiple_of((1 - x) * half, half)

    def forward(s):
        if s:
            arrived(19 + s)
            send(26 + s, slots.at[s], slots_s.at[s], sibling)

    sides = (slice(0, ff), slice(ff, 2 * ff))

    def stage_a(s):
        arrived(26 + s)
        for side, weights in zip(sides, (gate_all, up_all)):
            part_out[s, :, side] = project(s, theirs, weights).astype(BF16)
        send(30 + s, part_out.at[s], part_in.at[s], across)
        for side, weights in zip(sides, (gate_all, up_all)):
            part_own[s, :, side] = project(s, mine, weights)

    def stage_a_own(k):
        side, weights = sides[k], (gate_all, up_all)[k]
        part_out[0, :, side] = project(0, theirs, weights).astype(BF16)
        send(30 + 20 * k, part_out.at[0, :, side], part_in.at[0, :, side], across)
        part_own[0, :, side] = project(0, mine, weights)

    def stage_b(s):
        arrived(30 + s)
        if s == 0:
            arrived(50)
        gate_sum = part_own[s, :, :ff] + part_in[s, :, :ff].astype(F32)
        up_sum = part_own[s, :, ff:] + part_in[s, :, ff:].astype(F32)
        hidden[s, pl.ds(mine, half), :] = (silu(gate_sum) * up_sum).astype(BF16)
        kept = hidden.at[s, pl.ds(mine, half), :]
        send(34 + s, kept, kept, across)

    def stage_c(s):
        arrived(34 + s)
        if s:
            arrived(22 + s)
        columns = jnp.transpose(scale[s])
        weight = jnp.where(c == 0, columns[:, 0:1], columns[:, 1:2])
        units = hidden[s]
        half_out[s] = (dot(units, down_all[1 - c]) * weight).astype(BF16)
        send(38 + s, half_out.at[s], half_in.at[s], sibling)
        half_own[s] = dot(units, down_all[c]) * weight

    def stage_d(s):
        arrived(38 + s)
        both = (half_own[s] + half_in[s].astype(F32)).astype(BF16)
        if s == 0:
            back[0] = both
        else:
            back_out[s] = both
            send(41 + s, back_out.at[s], back.at[s], peer_of[s])

    weight_arrived(0)
    arrived(26)
    stage_a_own(0)
    dispatch(1)
    relay_arrived(2)
    relay_start(3)
    weight_arrived(1)
    stage_a_own(1)
    forward(2)
    arrived(10)
    send(11, normed.at[2], normed.at[3], sibling)
    stage_a(2)
    relay_arrived(3)
    send(18, branch_all.at[y], branch_all.at[y], pair)
    stage_b(0)
    forward(3)
    stage_a(3)
    stage_b(2)
    weight_arrived(2)
    stage_c(0)
    stage_d(0)
    forward(1)
    stage_a(1)
    stage_b(3)
    stage_c(2)
    stage_d(2)

    arrived(9)
    arrived(11)
    arrived(18)
    quarters = (tp, x * 2 + 1 - c, (1 - x) * 2 + c, (1 - x) * 2 + 1 - c)
    sums = jnp.zeros((token_count, block), F32)
    for k, q in enumerate(quarters):
        sums = sums + dot(normed[k, :, :block], branch_all[0, q, 0])
        sums = sums + dot(normed[k, :, block:], branch_all[1, q, 0])
    branch_hidden[...] = silu(sums).astype(BF16)

    def branch_part(q, side):
        return dot(branch_hidden[...], branch_all[side, q, 1])

    for side in range(2):
        columns = slice(side * block, (side + 1) * block)
        fold_out[0, :, columns] = branch_part(quarters[1], side).astype(BF16)
        fold_out[1, :, columns] = branch_part(quarters[3], side).astype(BF16)
    send(45, fold_out, fold_in, sibling)

    stage_b(1)
    stage_c(3)
    stage_d(3)

    arrived(45)
    for side in range(2):
        columns = slice(side * block, (side + 1) * block)
        cross_out[:, columns] = (
            branch_part(quarters[2], side) + fold_in[1, :, columns].astype(F32)
        ).astype(BF16)
    send(46, cross_out, cross_in, across)
    stage_c(1)
    stage_d(1)
    for side in range(2):
        columns = slice(side * block, (side + 1) * block)
        fold_own[:, columns] = branch_part(quarters[0], side) + fold_in[0, :, columns].astype(F32)

    slot_lane = lax.broadcasted_iota(jnp.int32, (token_count, capacity), 1)

    def restore(s):
        wanted = (slot_lane + level[s] * capacity).astype(F32)
        choose = jnp.where(wanted == code_col[:, 0:1], 1.0, 0.0).astype(BF16)
        return dot(choose, back[s])

    half_own_sum = restore(0)
    for s in (2, 3, 1):
        arrived(41 + s)
        half_own_sum = half_own_sum + restore(s)
    arrived(46)
    branch = fold_own[...] + cross_in[...].astype(F32)
    gate = 1.0 / (1.0 + jnp.exp(-branch_gate[...]))
    out[...] = (half_own_sum + gate * branch).astype(BF16)
    for copy in started.values():
        copy.wait_send()
    for hop in range(1, GROUPS):
        relay_sent(hop)
    for k in range(3):
        weight_copy(k, 0, pair_user).wait_send()

    @pl.when(c != y)
    def _():
        for k in range(3):
            weight_copy(k, 1, sibling).wait_send()


def pair_body(
    tokens,
    norm_gain,
    routing,
    route_weight,
    w_gate,
    w_up,
    w_down,
    w_branch_in,
    w_branch_out,
    branch_gate,
):
    count, quarter = tokens.shape
    ff = w_gate.shape[2]
    block = w_branch_in.shape[0]
    cap = count // 2
    half = cap // 2
    vmem = pltpu.VMEM
    rows = (GROUPS, cap, quarter)
    scratch = [
        vmem((2, quarter, ff), BF16),
        vmem((2, quarter, ff), BF16),
        vmem((2, ff, quarter), BF16),
        vmem((4, 8, count), F32),
        vmem((4, count, quarter), BF16),
        vmem((2, GROUPS, 2, block, block), BF16),
        vmem(rows, BF16),
        vmem(rows, BF16),
        vmem(rows, BF16),
        vmem((GROUPS, 8, cap), F32),
        vmem((GROUPS, 8, cap), F32),
        vmem((GROUPS, half, 2 * ff), BF16),
        vmem((GROUPS, half, 2 * ff), F32),
        vmem((GROUPS, half, 2 * ff), BF16),
        vmem((GROUPS, cap, ff), BF16),
        vmem(rows, BF16),
        vmem(rows, F32),
        vmem(rows, BF16),
        vmem(rows, BF16),
        vmem(rows, BF16),
        vmem((2, count, quarter), BF16),
        vmem((count, quarter), F32),
        vmem((2, count, quarter), BF16),
        vmem((count, quarter), BF16),
        vmem((count, quarter), BF16),
        vmem((count, block), BF16),
        vmem((count, 8), F32),
        pltpu.SemaphoreType.DMA((COPIES,)),
        pltpu.SemaphoreType.DMA((COPIES,)),
    ]
    return pl.pallas_call(
        pair_kernel,
        out_shape=jax.ShapeDtypeStruct((count, quarter), BF16),
        in_specs=[pl.BlockSpec(memory_space=vmem)] * 10,
        out_specs=pl.BlockSpec(memory_space=vmem),
        scratch_shapes=scratch,
        compiler_params=pltpu.CompilerParams(
            collective_id=0, has_side_effects=True, vmem_limit_bytes=60 * 1024 * 1024
        ),
    )(
        tokens,
        norm_gain[None, :],
        routing.T,
        route_weight.T,
        w_gate[0],
        w_up[0],
        w_down[0],
        w_branch_in,
        w_branch_out,
        branch_gate[None, :],
    )


def solution(mesh):
    return jax.shard_map(
        pair_body if mesh.shape["ep"] == 2 * GROUPS and mesh.shape["tp"] == 4 else body,
        mesh=mesh,
        in_specs=(
            P("ep", "tp"),
            P("tp"),
            P("ep", None),
            P("ep", None),
            P("ep", "tp", None),
            P("ep", "tp", None),
            P("ep", None, "tp"),
            P("ep", "tp"),
            P("tp", "ep"),
            P("tp"),
        ),
        out_specs=P("ep", "tp"),
        check_vma=False,
    )
```

```python
import functools

import jax
import jax.numpy as jnp
from jax import lax
from jax.experimental import pallas as pl
from jax.experimental.pallas import tpu as pltpu
from jax.sharding import PartitionSpec as P

GROUPS = 4


epsilon = 1e-06


def send_back(result):
    return lax.all_to_all(result, "ep", split_axis=0, concat_axis=0, tiled=True)


def body(
    tokens,
    norm_gain,
    routing,
    route_weight,
    w_gate,
    w_up,
    w_down,
    w_branch_in,
    w_branch_out,
    branch_gate,
):
    token_count, quarter = tokens.shape
    full_width = quarter * lax.axis_size("tp")
    floats = tokens.astype(jnp.float32)
    squares = lax.psum(jnp.sum(floats * floats, axis=1), "tp")
    normed = (floats * lax.rsqrt(squares[:, None] / full_width + epsilon) * norm_gain).astype(
        jnp.bfloat16
    )
    expert_count = lax.axis_size("ep") * w_gate.shape[0]
    capacity = token_count // (expert_count // GROUPS)
    flat_ids = routing.reshape(-1)
    one_hot = (flat_ids[:, None] == jnp.arange(expert_count, dtype=jnp.int32)[None, :]).astype(
        jnp.int32
    )
    before = jnp.cumsum(one_hot, axis=0) - one_hot
    position = flat_ids * capacity + jnp.sum(before * one_hot, axis=1)
    copies = jnp.repeat(normed, 2, axis=0)
    buffer = jnp.zeros((expert_count * capacity, quarter), jnp.bfloat16).at[position].set(copies)
    buffer = buffer.reshape(expert_count, capacity, quarter)
    gate_whole, up_whole, down_whole = (
        lax.all_gather(w_gate[0], "tp", axis=0, tiled=True),
        lax.all_gather(w_up[0], "tp", axis=0, tiled=True),
        lax.all_gather(w_down[0], "tp", axis=1, tiled=True),
    )
    row_split = lax.all_to_all(
        lax.all_to_all(buffer, "ep", split_axis=0, concat_axis=0, tiled=True),
        "tp",
        split_axis=0,
        concat_axis=2,
        tiled=True,
    )
    slot_rows = row_split.reshape(-1, row_split.shape[2])
    gate_sum = jnp.dot(slot_rows, gate_whole, preferred_element_type=jnp.float32)
    up_sum = jnp.dot(slot_rows, up_whole, preferred_element_type=jnp.float32)
    hidden = (jax.nn.silu(gate_sum) * up_sum).astype(jnp.bfloat16)
    result = jnp.dot(hidden, down_whole, preferred_element_type=jnp.float32).astype(jnp.bfloat16)
    feature_split = lax.all_to_all(
        result.reshape(row_split.shape), "tp", split_axis=2, concat_axis=0, tiled=True
    )
    returned = send_back(feature_split)
    picked = returned.reshape(expert_count * capacity, quarter)[position].reshape(
        token_count, 2, quarter
    )
    routed = jnp.sum(picked.astype(jnp.float32) * route_weight[:, :, None], axis=1)
    branch_tokens = lax.all_to_all(normed, "tp", split_axis=0, concat_axis=1, tiled=True)
    in_cols, out_rows = (
        lax.all_gather(w_branch_in, "tp", axis=1, tiled=True),
        lax.all_gather(w_branch_out, "tp", axis=0, tiled=True),
    )
    in_whole, out_whole = (
        lax.all_gather(in_cols, "ep", axis=0, tiled=True),
        lax.all_gather(out_rows, "ep", axis=1, tiled=True),
    )
    branch_hidden = jax.nn.silu(
        jnp.dot(branch_tokens, in_whole, preferred_element_type=jnp.float32)
    ).astype(jnp.bfloat16)
    branch_local = jnp.dot(branch_hidden, out_whole, preferred_element_type=jnp.float32).astype(
        jnp.bfloat16
    )
    branch = lax.all_to_all(branch_local, "tp", split_axis=1, concat_axis=0, tiled=True)
    return (routed + jax.nn.sigmoid(branch_gate) * branch.astype(jnp.float32)).astype(jnp.bfloat16)


BF16, F32 = jnp.bfloat16, jnp.float32
COPIES = 53


def dot(a, b):
    return jnp.dot(a, b, preferred_element_type=F32)


def dot_nt(a, b):
    return lax.dot_general(a, b, (((1,), (1,)), ((), ())), preferred_element_type=F32)


def silu(v):
    return v / (1.0 + jnp.exp(-v))


def pair_kernel(
    tokens,
    gain,
    routing,
    route_weight,
    w_gate,
    w_up,
    w_down,
    w_in,
    w_out,
    branch_gate,
    out,
    gate_all,
    up_all,
    down_all,
    squares,
    normed,
    branch_all,
    slots_out,
    slots,
    slots_s,
    scale_out,
    scale,
    part_out,
    part_own,
    part_in,
    hidden,
    half_out,
    half_own,
    half_in,
    back_out,
    back,
    fold_out,
    fold_own,
    fold_in,
    cross_out,
    cross_in,
    branch_hidden,
    code_col,
    send_sem,
    recv_sem,
):
    ep, tp = lax.axis_index("ep"), lax.axis_index("tp")
    z, y, x, c = ep // 2, ep % 2, tp // 2, tp % 2
    token_count, quarter = tokens.shape
    ff = w_gate.shape[1]
    capacity = slots.shape[1]
    half = capacity // 2
    block = w_in.shape[0]

    def at(zz, yy, xx, cc):
        return (zz * 2 + yy, xx * 2 + cc)

    sibling = at(z, y, x, 1 - c)
    across = at(z, y, 1 - x, c)
    diagonal = at(z, y, 1 - x, 1 - c)
    pair = at(z, 1 - y, x, c)
    pair_user = at(z, 1 - y, x, y)
    pair_other = at(z, 1 - y, x, 1 - c)
    level = [z, z + 1 - 2 * (z % 2), (z + 2) % GROUPS, GROUPS - 1 - z]
    peer_of = [None] + [at(level[m], y, x, c) for m in range(1, GROUPS)]
    up = at((z + 1) % GROUPS, y, x, c)
    down = at((z + GROUPS - 1) % GROUPS, y, x, c)

    barrier = pltpu.get_barrier_semaphore()
    peers = [sibling, across, diagonal, pair, pair_other] + peer_of[1:]
    for peer in peers:
        pl.semaphore_signal(
            barrier, inc=1, device_id=peer, device_id_type=pl.DeviceIdType.MESH
        )

    branch_all[y, z, 0] = w_in[...]
    branch_all[y, z, 1] = w_out[...]
    floats = tokens[...].astype(F32)
    exact = floats * floats
    high = exact.astype(BF16)
    low = (exact - high.astype(F32)).astype(BF16)
    ones = jnp.ones((16, quarter), BF16)
    squares[0] = (dot_nt(ones, high) + dot_nt(ones, low))[:8]

    pl.semaphore_wait(barrier, len(peers))

    started = {}

    def send(number, source, target, device):
        copy = pltpu.make_async_remote_copy(
            src_ref=source,
            dst_ref=target,
            send_sem=send_sem.at[number],
            recv_sem=recv_sem.at[number],
            device_id=device,
            device_id_type=pl.DeviceIdType.MESH,
        )
        copy.start()
        started[number] = copy

    def arrived(number):
        started[number].wait_recv()

    send(6, squares.at[0], squares.at[1], sibling)
    send(7, squares.at[0], squares.at[2], across)
    send(8, squares.at[0], squares.at[3], diagonal)

    weights_of = ((w_gate, gate_all), (w_up, up_all), (w_down, down_all))

    def weight_copy(k, sem, device):
        source, target = weights_of[k]
        return pltpu.make_async_remote_copy(
            src_ref=source,
            dst_ref=target.at[c],
            send_sem=send_sem.at[2 * k + sem],
            recv_sem=recv_sem.at[2 * k + c],
            device_id=device,
            device_id_type=pl.DeviceIdType.MESH,
        )

    for k in range(3):
        weight_copy(k, 0, pair_user).start()

    @pl.when(c != y)
    def _():
        for k in range(3):
            weight_copy(k, 1, sibling).start()

    @pl.when(c == y)
    def _():
        for source, target in weights_of:
            target[c] = source[...]

    def weight_arrived(k):
        source, target = weights_of[k]

        def wait(h):
            pltpu.make_async_remote_copy(
                src_ref=source,
                dst_ref=target.at[h],
                send_sem=send_sem.at[2 * k],
                recv_sem=recv_sem.at[2 * k + h],
                device_id=sibling,
                device_id_type=pl.DeviceIdType.MESH,
            ).wait_recv()

        wait(1 - c)

        @pl.when(c != y)
        def _():
            wait(c)

    def relay(hop, upward):
        number = (12 if upward else 47) + hop - 1
        held = z - (hop - 1) if upward else z + (hop - 1)
        came = z - hop if upward else z + hop
        held, came = (held + GROUPS) % GROUPS, (came + GROUPS) % GROUPS
        sends = (z <= GROUPS - 2) & (z >= hop - 1)
        gets = z >= hop
        if not upward:
            sends = (z >= 1) & (z <= GROUPS - hop)
            gets = z <= GROUPS - 1 - hop

        def copy(row):
            return pltpu.make_async_remote_copy(
                src_ref=branch_all.at[y, row],
                dst_ref=branch_all.at[y, row],
                send_sem=send_sem.at[number],
                recv_sem=recv_sem.at[number],
                device_id=up if upward else down,
                device_id_type=pl.DeviceIdType.MESH,
            )

        return sends, gets, lambda: copy(held), lambda: copy(came)

    def relay_start(hop):
        for upward in (True, False):
            sends, _, outgoing, _ = relay(hop, upward)

            @pl.when(sends)
            def _():
                outgoing().start()

    def relay_arrived(hop):
        for upward in (True, False):
            _, gets, _, incoming = relay(hop, upward)

            @pl.when(gets)
            def _():
                incoming().wait_recv()

    def relay_sent(hop):
        for upward in (True, False):
            sends, _, outgoing, _ = relay(hop, upward)

            @pl.when(sends)
            def _():
                outgoing().wait_send()

    relay_start(1)
    ids = routing[0:1, :]
    group = lax.shift_right_logical(ids, 1)
    rows16 = lax.broadcasted_iota(jnp.int32, (16, token_count), 0)
    member = jnp.where(rows16 == group, 1.0, 0.0)
    earlier = jnp.where(
        lax.broadcasted_iota(jnp.int32, (token_count, token_count), 0)
        < lax.broadcasted_iota(jnp.int32, (token_count, token_count), 1),
        1.0,
        0.0,
    ).astype(BF16)
    before = dot(member.astype(BF16), earlier)
    place = jnp.sum(member * before, axis=0, keepdims=True)
    code = group.astype(F32) * capacity + place
    code_col[...] = jnp.transpose(jnp.broadcast_to(code, (8, token_count)))
    first, second = route_weight[0:1, :], route_weight[1:2, :]
    even_first = (ids & 1) == 0
    for_even = jnp.where(even_first, first, second)
    for_odd = jnp.where(even_first, second, first)
    weights = jnp.where((rows16 & 1) == 0, for_even, for_odd)
    weights_high = weights.astype(BF16)
    weights_low = (weights - weights_high.astype(F32)).astype(BF16)

    for number in (6, 7, 8):
        arrived(number)
    total = squares[0] + squares[1] + squares[2] + squares[3]
    factor = lax.rsqrt(total / (4 * quarter) + epsilon)
    factor_col = jnp.transpose(factor)[:, 0:1]
    normed[0] = (tokens[...].astype(F32) * factor_col * gain[...]).astype(BF16)
    send(10, normed.at[0], normed.at[2], across)
    send(9, normed.at[0], normed.at[1], sibling)

    def dispatch(s):
        send(19 + s, slots_out.at[s], slots.at[s], peer_of[s])
        send(22 + s, scale_out.at[s], scale.at[s], peer_of[s])

    slot_row = lax.broadcasted_iota(jnp.int32, (capacity, token_count), 0)
    for s in (2, 3, 1, 0):
        wanted = (slot_row + level[s] * capacity).astype(F32)
        choose = jnp.where(wanted == code, 1.0, 0.0).astype(BF16)
        rows = dot(choose, normed[0]).astype(BF16)
        slot_weights = (dot_nt(weights_high, choose) + dot_nt(weights_low, choose))[:8]
        if s == 0:
            slots[0] = rows
            scale[0] = slot_weights
            send(26, slots.at[0], slots_s.at[0], sibling)
        else:
            slots_out[s] = rows
            scale_out[s] = slot_weights
            if s > 1:
                dispatch(s)

    def project(s, start, weights):
        own = slots[s, pl.ds(start, half), :]
        other = slots_s[s, pl.ds(start, half), :]
        return dot(own, weights[c]) + dot(other, weights[1 - c])

    mine = pl.multiple_of(x * half, half)
    theirs = pl.multiple_of((1 - x) * half, half)

    def forward(s):
        if s:
            arrived(19 + s)
            send(26 + s, slots.at[s], slots_s.at[s], sibling)

    sides = (slice(0, ff), slice(ff, 2 * ff))

    def stage_a(s):
        arrived(26 + s)
        for side, weights in zip(sides, (gate_all, up_all)):
            part_out[s, :, side] = project(s, theirs, weights).astype(BF16)
        send(30 + s, part_out.at[s], part_in.at[s], across)
        for side, weights in zip(sides, (gate_all, up_all)):
            part_own[s, :, side] = project(s, mine, weights)

    def stage_a_own(k):
        side, weights = sides[k], (gate_all, up_all)[k]
        part_out[0, :, side] = project(0, theirs, weights).astype(BF16)
        send(30 + 20 * k, part_out.at[0, :, side], part_in.at[0, :, side], across)
        part_own[0, :, side] = project(0, mine, weights)

    def stage_b(s):
        arrived(30 + s)
        if s == 0:
            arrived(50)
        gate_sum = part_own[s, :, :ff] + part_in[s, :, :ff].astype(F32)
        up_sum = part_own[s, :, ff:] + part_in[s, :, ff:].astype(F32)
        hidden[s, pl.ds(mine, half), :] = (silu(gate_sum) * up_sum).astype(BF16)
        kept = hidden.at[s, pl.ds(mine, half), :]
        send(34 + s, kept, kept, across)

    def stage_c(s):
        arrived(34 + s)
        if s:
            arrived(22 + s)
        columns = jnp.transpose(scale[s])
        weight = jnp.where(c == 0, columns[:, 0:1], columns[:, 1:2])
        units = hidden[s]
        half_out[s] = (dot(units, down_all[1 - c]) * weight).astype(BF16)
        send(38 + s, half_out.at[s], half_in.at[s], sibling)
        half_own[s] = dot(units, down_all[c]) * weight

    def stage_d(s):
        arrived(38 + s)
        both = (half_own[s] + half_in[s].astype(F32)).astype(BF16)
        if s == 0:
            back[0] = both
        else:
            back_out[s] = both
            send(41 + s, back_out.at[s], back.at[s], peer_of[s])

    weight_arrived(0)
    arrived(26)
    stage_a_own(0)
    weight_arrived(1)
    stage_a_own(1)
    dispatch(1)
    relay_arrived(1)
    relay_start(2)
    forward(2)
    stage_a(2)
    arrived(10)
    send(11, normed.at[2], normed.at[3], sibling)
    relay_arrived(2)
    relay_start(3)
    forward(3)
    stage_a(3)
    stage_b(2)
    relay_arrived(3)
    send(18, branch_all.at[y], branch_all.at[y], pair)
    stage_b(3)
    stage_b(0)
    weight_arrived(2)
    stage_c(2)
    forward(1)
    stage_a(1)
    stage_d(2)
    stage_c(3)
    stage_c(0)
    stage_d(3)
    stage_d(0)

    arrived(9)
    arrived(11)
    arrived(18)
    quarters = (tp, x * 2 + 1 - c, (1 - x) * 2 + c, (1 - x) * 2 + 1 - c)
    sums = jnp.zeros((token_count, block), F32)
    for k, q in enumerate(quarters):
        sums = sums + dot(normed[k, :, :block], branch_all[0, q, 0])
        sums = sums + dot(normed[k, :, block:], branch_all[1, q, 0])
    branch_hidden[...] = silu(sums).astype(BF16)

    def branch_part(q, side):
        return dot(branch_hidden[...], branch_all[side, q, 1])

    for side in range(2):
        columns = slice(side * block, (side + 1) * block)
        fold_out[0, :, columns] = branch_part(quarters[1], side).astype(BF16)
        fold_out[1, :, columns] = branch_part(quarters[3], side).astype(BF16)
    send(45, fold_out, fold_in, sibling)

    stage_b(1)

    arrived(45)
    for side in range(2):
        columns = slice(side * block, (side + 1) * block)
        cross_out[:, columns] = (
            branch_part(quarters[2], side) + fold_in[1, :, columns].astype(F32)
        ).astype(BF16)
    send(46, cross_out, cross_in, across)
    stage_c(1)
    stage_d(1)
    for side in range(2):
        columns = slice(side * block, (side + 1) * block)
        fold_own[:, columns] = branch_part(quarters[0], side) + fold_in[0, :, columns].astype(F32)

    slot_lane = lax.broadcasted_iota(jnp.int32, (token_count, capacity), 1)

    def restore(s):
        wanted = (slot_lane + level[s] * capacity).astype(F32)
        choose = jnp.where(wanted == code_col[:, 0:1], 1.0, 0.0).astype(BF16)
        return dot(choose, back[s])

    half_own_sum = restore(0)
    for s in (2, 3, 1):
        arrived(41 + s)
        half_own_sum = half_own_sum + restore(s)
    arrived(46)
    branch = fold_own[...] + cross_in[...].astype(F32)
    gate = 1.0 / (1.0 + jnp.exp(-branch_gate[...]))
    out[...] = (half_own_sum + gate * branch).astype(BF16)
    for copy in started.values():
        copy.wait_send()
    for hop in range(1, GROUPS):
        relay_sent(hop)
    for k in range(3):
        weight_copy(k, 0, pair_user).wait_send()

    @pl.when(c != y)
    def _():
        for k in range(3):
            weight_copy(k, 1, sibling).wait_send()


def pair_body(
    tokens,
    norm_gain,
    routing,
    route_weight,
    w_gate,
    w_up,
    w_down,
    w_branch_in,
    w_branch_out,
    branch_gate,
):
    count, quarter = tokens.shape
    ff = w_gate.shape[2]
    block = w_branch_in.shape[0]
    cap = count // 2
    half = cap // 2
    vmem = pltpu.VMEM
    rows = (GROUPS, cap, quarter)
    scratch = [
        vmem((2, quarter, ff), BF16),
        vmem((2, quarter, ff), BF16),
        vmem((2, ff, quarter), BF16),
        vmem((4, 8, count), F32),
        vmem((4, count, quarter), BF16),
        vmem((2, GROUPS, 2, block, block), BF16),
        vmem(rows, BF16),
        vmem(rows, BF16),
        vmem(rows, BF16),
        vmem((GROUPS, 8, cap), F32),
        vmem((GROUPS, 8, cap), F32),
        vmem((GROUPS, half, 2 * ff), BF16),
        vmem((GROUPS, half, 2 * ff), F32),
        vmem((GROUPS, half, 2 * ff), BF16),
        vmem((GROUPS, cap, ff), BF16),
        vmem(rows, BF16),
        vmem(rows, F32),
        vmem(rows, BF16),
        vmem(rows, BF16),
        vmem(rows, BF16),
        vmem((2, count, quarter), BF16),
        vmem((count, quarter), F32),
        vmem((2, count, quarter), BF16),
        vmem((count, quarter), BF16),
        vmem((count, quarter), BF16),
        vmem((count, block), BF16),
        vmem((count, 8), F32),
        pltpu.SemaphoreType.DMA((COPIES,)),
        pltpu.SemaphoreType.DMA((COPIES,)),
    ]
    return pl.pallas_call(
        pair_kernel,
        out_shape=jax.ShapeDtypeStruct((count, quarter), BF16),
        in_specs=[pl.BlockSpec(memory_space=vmem)] * 10,
        out_specs=pl.BlockSpec(memory_space=vmem),
        scratch_shapes=scratch,
        compiler_params=pltpu.CompilerParams(
            collective_id=0, has_side_effects=True, vmem_limit_bytes=60 * 1024 * 1024
        ),
    )(
        tokens,
        norm_gain[None, :],
        routing.T,
        route_weight.T,
        w_gate[0],
        w_up[0],
        w_down[0],
        w_branch_in,
        w_branch_out,
        branch_gate[None, :],
    )


def solution(mesh):
    return jax.shard_map(
        pair_body if mesh.shape["ep"] == 2 * GROUPS and mesh.shape["tp"] == 4 else body,
        mesh=mesh,
        in_specs=(
            P("ep", "tp"),
            P("tp"),
            P("ep", None),
            P("ep", None),
            P("ep", "tp", None),
            P("ep", "tp", None),
            P("ep", None, "tp"),
            P("ep", "tp"),
            P("tp", "ep"),
            P("tp"),
        ),
        out_specs=P("ep", "tp"),
        check_vma=False,
    )
```

```python
import functools

import jax
import jax.numpy as jnp
from jax import lax
from jax.experimental import pallas as pl
from jax.experimental.pallas import tpu as pltpu
from jax.sharding import PartitionSpec as P

GROUPS = 4


epsilon = 1e-06


def send_back(result):
    return lax.all_to_all(result, "ep", split_axis=0, concat_axis=0, tiled=True)


def body(
    tokens,
    norm_gain,
    routing,
    route_weight,
    w_gate,
    w_up,
    w_down,
    w_branch_in,
    w_branch_out,
    branch_gate,
):
    token_count, quarter = tokens.shape
    full_width = quarter * lax.axis_size("tp")
    floats = tokens.astype(jnp.float32)
    squares = lax.psum(jnp.sum(floats * floats, axis=1), "tp")
    normed = (floats * lax.rsqrt(squares[:, None] / full_width + epsilon) * norm_gain).astype(
        jnp.bfloat16
    )
    expert_count = lax.axis_size("ep") * w_gate.shape[0]
    capacity = token_count // (expert_count // GROUPS)
    flat_ids = routing.reshape(-1)
    one_hot = (flat_ids[:, None] == jnp.arange(expert_count, dtype=jnp.int32)[None, :]).astype(
        jnp.int32
    )
    before = jnp.cumsum(one_hot, axis=0) - one_hot
    position = flat_ids * capacity + jnp.sum(before * one_hot, axis=1)
    copies = jnp.repeat(normed, 2, axis=0)
    buffer = jnp.zeros((expert_count * capacity, quarter), jnp.bfloat16).at[position].set(copies)
    buffer = buffer.reshape(expert_count, capacity, quarter)
    gate_whole, up_whole, down_whole = (
        lax.all_gather(w_gate[0], "tp", axis=0, tiled=True),
        lax.all_gather(w_up[0], "tp", axis=0, tiled=True),
        lax.all_gather(w_down[0], "tp", axis=1, tiled=True),
    )
    row_split = lax.all_to_all(
        lax.all_to_all(buffer, "ep", split_axis=0, concat_axis=0, tiled=True),
        "tp",
        split_axis=0,
        concat_axis=2,
        tiled=True,
    )
    slot_rows = row_split.reshape(-1, row_split.shape[2])
    gate_sum = jnp.dot(slot_rows, gate_whole, preferred_element_type=jnp.float32)
    up_sum = jnp.dot(slot_rows, up_whole, preferred_element_type=jnp.float32)
    hidden = (jax.nn.silu(gate_sum) * up_sum).astype(jnp.bfloat16)
    result = jnp.dot(hidden, down_whole, preferred_element_type=jnp.float32).astype(jnp.bfloat16)
    feature_split = lax.all_to_all(
        result.reshape(row_split.shape), "tp", split_axis=2, concat_axis=0, tiled=True
    )
    returned = send_back(feature_split)
    picked = returned.reshape(expert_count * capacity, quarter)[position].reshape(
        token_count, 2, quarter
    )
    routed = jnp.sum(picked.astype(jnp.float32) * route_weight[:, :, None], axis=1)
    branch_tokens = lax.all_to_all(normed, "tp", split_axis=0, concat_axis=1, tiled=True)
    in_cols, out_rows = (
        lax.all_gather(w_branch_in, "tp", axis=1, tiled=True),
        lax.all_gather(w_branch_out, "tp", axis=0, tiled=True),
    )
    in_whole, out_whole = (
        lax.all_gather(in_cols, "ep", axis=0, tiled=True),
        lax.all_gather(out_rows, "ep", axis=1, tiled=True),
    )
    branch_hidden = jax.nn.silu(
        jnp.dot(branch_tokens, in_whole, preferred_element_type=jnp.float32)
    ).astype(jnp.bfloat16)
    branch_local = jnp.dot(branch_hidden, out_whole, preferred_element_type=jnp.float32).astype(
        jnp.bfloat16
    )
    branch = lax.all_to_all(branch_local, "tp", split_axis=1, concat_axis=0, tiled=True)
    return (routed + jax.nn.sigmoid(branch_gate) * branch.astype(jnp.float32)).astype(jnp.bfloat16)


BF16, F32 = jnp.bfloat16, jnp.float32
COPIES = 53


def dot(a, b):
    return jnp.dot(a, b, preferred_element_type=F32)


def dot_nt(a, b):
    return lax.dot_general(a, b, (((1,), (1,)), ((), ())), preferred_element_type=F32)


def silu(v):
    return v / (1.0 + jnp.exp(-v))


def pair_kernel(
    tokens,
    gain,
    routing,
    route_weight,
    w_gate,
    w_up,
    w_down,
    w_in,
    w_out,
    branch_gate,
    out,
    gate_all,
    up_all,
    down_all,
    squares,
    normed,
    branch_all,
    slots_out,
    slots,
    slots_s,
    scale_out,
    scale,
    part_out,
    part_own,
    part_in,
    hidden,
    half_out,
    half_own,
    half_in,
    back_out,
    back,
    fold_out,
    fold_own,
    fold_in,
    cross_out,
    cross_in,
    branch_hidden,
    code_col,
    send_sem,
    recv_sem,
):
    ep, tp = lax.axis_index("ep"), lax.axis_index("tp")
    z, y, x, c = ep // 2, ep % 2, tp // 2, tp % 2
    token_count, quarter = tokens.shape
    ff = w_gate.shape[1]
    capacity = slots.shape[1]
    half = capacity // 2
    block = w_in.shape[0]

    def at(zz, yy, xx, cc):
        return (zz * 2 + yy, xx * 2 + cc)

    sibling = at(z, y, x, 1 - c)
    across = at(z, y, 1 - x, c)
    diagonal = at(z, y, 1 - x, 1 - c)
    pair = at(z, 1 - y, x, c)
    pair_user = at(z, 1 - y, x, y)
    pair_other = at(z, 1 - y, x, 1 - c)
    level = [z, z + 1 - 2 * (z % 2), (z + 2) % GROUPS, GROUPS - 1 - z]
    peer_of = [None] + [at(level[m], y, x, c) for m in range(1, GROUPS)]
    up = at((z + 1) % GROUPS, y, x, c)
    down = at((z + GROUPS - 1) % GROUPS, y, x, c)

    barrier = pltpu.get_barrier_semaphore()
    peers = [sibling, across, diagonal, pair, pair_other] + peer_of[1:]
    for peer in peers:
        pl.semaphore_signal(
            barrier, inc=1, device_id=peer, device_id_type=pl.DeviceIdType.MESH
        )

    branch_all[y, z, 0] = w_in[...]
    branch_all[y, z, 1] = w_out[...]
    floats = tokens[...].astype(F32)
    exact = floats * floats
    high = exact.astype(BF16)
    low = (exact - high.astype(F32)).astype(BF16)
    ones = jnp.ones((16, quarter), BF16)
    squares[0] = (dot_nt(ones, high) + dot_nt(ones, low))[:8]

    pl.semaphore_wait(barrier, len(peers))

    started = {}

    def send(number, source, target, device):
        copy = pltpu.make_async_remote_copy(
            src_ref=source,
            dst_ref=target,
            send_sem=send_sem.at[number],
            recv_sem=recv_sem.at[number],
            device_id=device,
            device_id_type=pl.DeviceIdType.MESH,
        )
        copy.start()
        started[number] = copy

    def arrived(number):
        started[number].wait_recv()

    send(6, squares.at[0], squares.at[1], sibling)
    send(7, squares.at[0], squares.at[2], across)
    send(8, squares.at[0], squares.at[3], diagonal)

    weights_of = ((w_gate, gate_all), (w_up, up_all), (w_down, down_all))

    def weight_copy(k, sem, device):
        source, target = weights_of[k]
        return pltpu.make_async_remote_copy(
            src_ref=source,
            dst_ref=target.at[c],
            send_sem=send_sem.at[2 * k + sem],
            recv_sem=recv_sem.at[2 * k + c],
            device_id=device,
            device_id_type=pl.DeviceIdType.MESH,
        )

    for k in range(3):
        weight_copy(k, 0, pair_user).start()

    @pl.when(c != y)
    def _():
        for k in range(3):
            weight_copy(k, 1, sibling).start()

    @pl.when(c == y)
    def _():
        for source, target in weights_of:
            target[c] = source[...]

    def weight_arrived(k):
        source, target = weights_of[k]

        def wait(h):
            pltpu.make_async_remote_copy(
                src_ref=source,
                dst_ref=target.at[h],
                send_sem=send_sem.at[2 * k],
                recv_sem=recv_sem.at[2 * k + h],
                device_id=sibling,
                device_id_type=pl.DeviceIdType.MESH,
            ).wait_recv()

        wait(1 - c)

        @pl.when(c != y)
        def _():
            wait(c)

    def relay(hop, upward):
        number = (12 if upward else 47) + hop - 1
        held = z - (hop - 1) if upward else z + (hop - 1)
        came = z - hop if upward else z + hop
        held, came = (held + GROUPS) % GROUPS, (came + GROUPS) % GROUPS
        sends = (z <= GROUPS - 2) & (z >= hop - 1)
        gets = z >= hop
        if not upward:
            sends = (z >= 1) & (z <= GROUPS - hop)
            gets = z <= GROUPS - 1 - hop

        def copy(row):
            return pltpu.make_async_remote_copy(
                src_ref=branch_all.at[y, row],
                dst_ref=branch_all.at[y, row],
                send_sem=send_sem.at[number],
                recv_sem=recv_sem.at[number],
                device_id=up if upward else down,
                device_id_type=pl.DeviceIdType.MESH,
            )

        return sends, gets, lambda: copy(held), lambda: copy(came)

    def relay_start(hop):
        for upward in (True, False):
            sends, _, outgoing, _ = relay(hop, upward)

            @pl.when(sends)
            def _():
                outgoing().start()

    def relay_arrived(hop):
        for upward in (True, False):
            _, gets, _, incoming = relay(hop, upward)

            @pl.when(gets)
            def _():
                incoming().wait_recv()

    def relay_sent(hop):
        for upward in (True, False):
            sends, _, outgoing, _ = relay(hop, upward)

            @pl.when(sends)
            def _():
                outgoing().wait_send()

    relay_start(1)
    ids = routing[0:1, :]
    group = lax.shift_right_logical(ids, 1)
    rows16 = lax.broadcasted_iota(jnp.int32, (16, token_count), 0)
    member = jnp.where(rows16 == group, 1.0, 0.0)
    earlier = jnp.where(
        lax.broadcasted_iota(jnp.int32, (token_count, token_count), 0)
        < lax.broadcasted_iota(jnp.int32, (token_count, token_count), 1),
        1.0,
        0.0,
    ).astype(BF16)
    before = dot(member.astype(BF16), earlier)
    place = jnp.sum(member * before, axis=0, keepdims=True)
    code = group.astype(F32) * capacity + place
    code_col[...] = jnp.transpose(jnp.broadcast_to(code, (8, token_count)))
    first, second = route_weight[0:1, :], route_weight[1:2, :]
    even_first = (ids & 1) == 0
    for_even = jnp.where(even_first, first, second)
    for_odd = jnp.where(even_first, second, first)
    weights = jnp.where((rows16 & 1) == 0, for_even, for_odd)
    weights_high = weights.astype(BF16)
    weights_low = (weights - weights_high.astype(F32)).astype(BF16)

    for number in (6, 7, 8):
        arrived(number)
    total = squares[0] + squares[1] + squares[2] + squares[3]
    factor = lax.rsqrt(total / (4 * quarter) + epsilon)
    factor_col = jnp.transpose(factor)[:, 0:1]
    normed[0] = (tokens[...].astype(F32) * factor_col * gain[...]).astype(BF16)
    send(10, normed.at[0], normed.at[2], across)
    send(9, normed.at[0], normed.at[1], sibling)

    def dispatch(s):
        send(19 + s, slots_out.at[s], slots.at[s], peer_of[s])
        send(22 + s, scale_out.at[s], scale.at[s], peer_of[s])

    slot_row = lax.broadcasted_iota(jnp.int32, (capacity, token_count), 0)
    for s in (2, 3, 1, 0):
        wanted = (slot_row + level[s] * capacity).astype(F32)
        choose = jnp.where(wanted == code, 1.0, 0.0).astype(BF16)
        rows = dot(choose, normed[0]).astype(BF16)
        slot_weights = (dot_nt(weights_high, choose) + dot_nt(weights_low, choose))[:8]
        if s == 0:
            slots[0] = rows
            scale[0] = slot_weights
            send(26, slots.at[0], slots_s.at[0], sibling)
        else:
            slots_out[s] = rows
            scale_out[s] = slot_weights
            if s > 1:
                dispatch(s)

    def project(s, start, weights):
        own = slots[s, pl.ds(start, half), :]
        other = slots_s[s, pl.ds(start, half), :]
        return dot(own, weights[c]) + dot(other, weights[1 - c])

    mine = pl.multiple_of(x * half, half)
    theirs = pl.multiple_of((1 - x) * half, half)

    def forward(s):
        if s:
            arrived(19 + s)
            send(26 + s, slots.at[s], slots_s.at[s], sibling)

    sides = (slice(0, ff), slice(ff, 2 * ff))

    def stage_a(s):
        arrived(26 + s)
        for side, weights in zip(sides, (gate_all, up_all)):
            part_out[s, :, side] = project(s, theirs, weights).astype(BF16)
        send(30 + s, part_out.at[s], part_in.at[s], across)
        for side, weights in zip(sides, (gate_all, up_all)):
            part_own[s, :, side] = project(s, mine, weights)

    def stage_a_own(k):
        side, weights = sides[k], (gate_all, up_all)[k]
        part_out[0, :, side] = project(0, theirs, weights).astype(BF16)
        send(30 + 20 * k, part_out.at[0, :, side], part_in.at[0, :, side], across)
        part_own[0, :, side] = project(0, mine, weights)

    def stage_b(s):
        arrived(30 + s)
        if s == 0:
            arrived(50)
        gate_sum = part_own[s, :, :ff] + part_in[s, :, :ff].astype(F32)
        up_sum = part_own[s, :, ff:] + part_in[s, :, ff:].astype(F32)
        hidden[s, pl.ds(mine, half), :] = (silu(gate_sum) * up_sum).astype(BF16)
        kept = hidden.at[s, pl.ds(mine, half), :]
        send(34 + s, kept, kept, across)

    def stage_c(s):
        arrived(34 + s)
        if s:
            arrived(22 + s)
        columns = jnp.transpose(scale[s])
        weight = jnp.where(c == 0, columns[:, 0:1], columns[:, 1:2])
        units = hidden[s]
        half_out[s] = (dot(units, down_all[1 - c]) * weight).astype(BF16)
        send(38 + s, half_out.at[s], half_in.at[s], sibling)
        half_own[s] = dot(units, down_all[c]) * weight

    def stage_d(s):
        arrived(38 + s)
        both = (half_own[s] + half_in[s].astype(F32)).astype(BF16)
        if s == 0:
            back[0] = both
        else:
            back_out[s] = both
            send(41 + s, back_out.at[s], back.at[s], peer_of[s])

    def pair_send(m):
        rows = branch_all.at[y, level[m]]
        send(15 + m, rows, rows, pair)

    weight_arrived(0)
    arrived(26)
    stage_a_own(0)
    weight_arrived(1)
    stage_a_own(1)
    dispatch(1)
    relay_arrived(1)
    relay_start(2)
    pair_send(0)
    pair_send(1)
    forward(2)
    stage_a(2)
    arrived(10)
    send(11, normed.at[2], normed.at[3], sibling)
    forward(3)
    stage_a(3)
    relay_arrived(2)
    relay_start(3)
    pair_send(2)
    stage_b(2)
    stage_b(3)
    stage_b(0)
    relay_arrived(3)
    pair_send(3)
    weight_arrived(2)
    stage_c(2)
    forward(1)
    stage_a(1)
    stage_d(2)
    stage_c(3)
    stage_c(0)
    stage_d(3)
    stage_d(0)

    arrived(9)
    arrived(11)
    for m in range(GROUPS):
        arrived(15 + m)
    quarters = (tp, x * 2 + 1 - c, (1 - x) * 2 + c, (1 - x) * 2 + 1 - c)
    sums = jnp.zeros((token_count, block), F32)
    for k, q in enumerate(quarters):
        sums = sums + dot(normed[k, :, :block], branch_all[0, q, 0])
        sums = sums + dot(normed[k, :, block:], branch_all[1, q, 0])
    branch_hidden[...] = silu(sums).astype(BF16)

    def branch_part(q, side):
        return dot(branch_hidden[...], branch_all[side, q, 1])

    for side in range(2):
        columns = slice(side * block, (side + 1) * block)
        fold_out[0, :, columns] = branch_part(quarters[1], side).astype(BF16)
        fold_out[1, :, columns] = branch_part(quarters[3], side).astype(BF16)
    send(45, fold_out, fold_in, sibling)

    stage_b(1)

    arrived(45)
    for side in range(2):
        columns = slice(side * block, (side + 1) * block)
        cross_out[:, columns] = (
            branch_part(quarters[2], side) + fold_in[1, :, columns].astype(F32)
        ).astype(BF16)
    send(46, cross_out, cross_in, across)
    stage_c(1)
    stage_d(1)
    for side in range(2):
        columns = slice(side * block, (side + 1) * block)
        fold_own[:, columns] = branch_part(quarters[0], side) + fold_in[0, :, columns].astype(F32)

    slot_lane = lax.broadcasted_iota(jnp.int32, (token_count, capacity), 1)

    def restore(s):
        wanted = (slot_lane + level[s] * capacity).astype(F32)
        choose = jnp.where(wanted == code_col[:, 0:1], 1.0, 0.0).astype(BF16)
        return dot(choose, back[s])

    half_own_sum = restore(0)
    for s in (2, 3, 1):
        arrived(41 + s)
        half_own_sum = half_own_sum + restore(s)
    arrived(46)
    branch = fold_own[...] + cross_in[...].astype(F32)
    gate = 1.0 / (1.0 + jnp.exp(-branch_gate[...]))
    out[...] = (half_own_sum + gate * branch).astype(BF16)
    for copy in started.values():
        copy.wait_send()
    for hop in range(1, GROUPS):
        relay_sent(hop)
    for k in range(3):
        weight_copy(k, 0, pair_user).wait_send()

    @pl.when(c != y)
    def _():
        for k in range(3):
            weight_copy(k, 1, sibling).wait_send()


def pair_body(
    tokens,
    norm_gain,
    routing,
    route_weight,
    w_gate,
    w_up,
    w_down,
    w_branch_in,
    w_branch_out,
    branch_gate,
):
    count, quarter = tokens.shape
    ff = w_gate.shape[2]
    block = w_branch_in.shape[0]
    cap = count // 2
    half = cap // 2
    vmem = pltpu.VMEM
    rows = (GROUPS, cap, quarter)
    scratch = [
        vmem((2, quarter, ff), BF16),
        vmem((2, quarter, ff), BF16),
        vmem((2, ff, quarter), BF16),
        vmem((4, 8, count), F32),
        vmem((4, count, quarter), BF16),
        vmem((2, GROUPS, 2, block, block), BF16),
        vmem(rows, BF16),
        vmem(rows, BF16),
        vmem(rows, BF16),
        vmem((GROUPS, 8, cap), F32),
        vmem((GROUPS, 8, cap), F32),
        vmem((GROUPS, half, 2 * ff), BF16),
        vmem((GROUPS, half, 2 * ff), F32),
        vmem((GROUPS, half, 2 * ff), BF16),
        vmem((GROUPS, cap, ff), BF16),
        vmem(rows, BF16),
        vmem(rows, F32),
        vmem(rows, BF16),
        vmem(rows, BF16),
        vmem(rows, BF16),
        vmem((2, count, quarter), BF16),
        vmem((count, quarter), F32),
        vmem((2, count, quarter), BF16),
        vmem((count, quarter), BF16),
        vmem((count, quarter), BF16),
        vmem((count, block), BF16),
        vmem((count, 8), F32),
        pltpu.SemaphoreType.DMA((COPIES,)),
        pltpu.SemaphoreType.DMA((COPIES,)),
    ]
    return pl.pallas_call(
        pair_kernel,
        out_shape=jax.ShapeDtypeStruct((count, quarter), BF16),
        in_specs=[pl.BlockSpec(memory_space=vmem)] * 10,
        out_specs=pl.BlockSpec(memory_space=vmem),
        scratch_shapes=scratch,
        compiler_params=pltpu.CompilerParams(
            collective_id=0, has_side_effects=True, vmem_limit_bytes=60 * 1024 * 1024
        ),
    )(
        tokens,
        norm_gain[None, :],
        routing.T,
        route_weight.T,
        w_gate[0],
        w_up[0],
        w_down[0],
        w_branch_in,
        w_branch_out,
        branch_gate[None, :],
    )


def solution(mesh):
    return jax.shard_map(
        pair_body if mesh.shape["ep"] == 2 * GROUPS and mesh.shape["tp"] == 4 else body,
        mesh=mesh,
        in_specs=(
            P("ep", "tp"),
            P("tp"),
            P("ep", None),
            P("ep", None),
            P("ep", "tp", None),
            P("ep", "tp", None),
            P("ep", None, "tp"),
            P("ep", "tp"),
            P("tp", "ep"),
            P("tp"),
        ),
        out_specs=P("ep", "tp"),
        check_vma=False,
    )
```

```python
import functools

import jax
import jax.numpy as jnp
from jax import lax
from jax.experimental import pallas as pl
from jax.experimental.pallas import tpu as pltpu
from jax.sharding import PartitionSpec as P

GROUPS = 4


epsilon = 1e-06


def send_back(result):
    return lax.all_to_all(result, "ep", split_axis=0, concat_axis=0, tiled=True)


def body(
    tokens,
    norm_gain,
    routing,
    route_weight,
    w_gate,
    w_up,
    w_down,
    w_branch_in,
    w_branch_out,
    branch_gate,
):
    token_count, quarter = tokens.shape
    full_width = quarter * lax.axis_size("tp")
    floats = tokens.astype(jnp.float32)
    squares = lax.psum(jnp.sum(floats * floats, axis=1), "tp")
    normed = (floats * lax.rsqrt(squares[:, None] / full_width + epsilon) * norm_gain).astype(
        jnp.bfloat16
    )
    expert_count = lax.axis_size("ep") * w_gate.shape[0]
    capacity = token_count // (expert_count // GROUPS)
    flat_ids = routing.reshape(-1)
    one_hot = (flat_ids[:, None] == jnp.arange(expert_count, dtype=jnp.int32)[None, :]).astype(
        jnp.int32
    )
    before = jnp.cumsum(one_hot, axis=0) - one_hot
    position = flat_ids * capacity + jnp.sum(before * one_hot, axis=1)
    copies = jnp.repeat(normed, 2, axis=0)
    buffer = jnp.zeros((expert_count * capacity, quarter), jnp.bfloat16).at[position].set(copies)
    buffer = buffer.reshape(expert_count, capacity, quarter)
    gate_whole, up_whole, down_whole = (
        lax.all_gather(w_gate[0], "tp", axis=0, tiled=True),
        lax.all_gather(w_up[0], "tp", axis=0, tiled=True),
        lax.all_gather(w_down[0], "tp", axis=1, tiled=True),
    )
    row_split = lax.all_to_all(
        lax.all_to_all(buffer, "ep", split_axis=0, concat_axis=0, tiled=True),
        "tp",
        split_axis=0,
        concat_axis=2,
        tiled=True,
    )
    slot_rows = row_split.reshape(-1, row_split.shape[2])
    gate_sum = jnp.dot(slot_rows, gate_whole, preferred_element_type=jnp.float32)
    up_sum = jnp.dot(slot_rows, up_whole, preferred_element_type=jnp.float32)
    hidden = (jax.nn.silu(gate_sum) * up_sum).astype(jnp.bfloat16)
    result = jnp.dot(hidden, down_whole, preferred_element_type=jnp.float32).astype(jnp.bfloat16)
    feature_split = lax.all_to_all(
        result.reshape(row_split.shape), "tp", split_axis=2, concat_axis=0, tiled=True
    )
    returned = send_back(feature_split)
    picked = returned.reshape(expert_count * capacity, quarter)[position].reshape(
        token_count, 2, quarter
    )
    routed = jnp.sum(picked.astype(jnp.float32) * route_weight[:, :, None], axis=1)
    branch_tokens = lax.all_to_all(normed, "tp", split_axis=0, concat_axis=1, tiled=True)
    in_cols, out_rows = (
        lax.all_gather(w_branch_in, "tp", axis=1, tiled=True),
        lax.all_gather(w_branch_out, "tp", axis=0, tiled=True),
    )
    in_whole, out_whole = (
        lax.all_gather(in_cols, "ep", axis=0, tiled=True),
        lax.all_gather(out_rows, "ep", axis=1, tiled=True),
    )
    branch_hidden = jax.nn.silu(
        jnp.dot(branch_tokens, in_whole, preferred_element_type=jnp.float32)
    ).astype(jnp.bfloat16)
    branch_local = jnp.dot(branch_hidden, out_whole, preferred_element_type=jnp.float32).astype(
        jnp.bfloat16
    )
    branch = lax.all_to_all(branch_local, "tp", split_axis=1, concat_axis=0, tiled=True)
    return (routed + jax.nn.sigmoid(branch_gate) * branch.astype(jnp.float32)).astype(jnp.bfloat16)


BF16, F32 = jnp.bfloat16, jnp.float32
COPIES = 53


def dot(a, b):
    return jnp.dot(a, b, preferred_element_type=F32)


def dot_nt(a, b):
    return lax.dot_general(a, b, (((1,), (1,)), ((), ())), preferred_element_type=F32)


def silu(v):
    return v / (1.0 + jnp.exp(-v))


def pair_kernel(
    tokens,
    gain,
    routing,
    route_weight,
    w_gate,
    w_up,
    w_down,
    w_in,
    w_out,
    branch_gate,
    out,
    gate_all,
    up_all,
    down_all,
    squares,
    normed,
    branch_all,
    slots_out,
    slots,
    slots_s,
    scale_out,
    scale,
    part_out,
    part_own,
    part_in,
    hidden,
    half_out,
    half_own,
    half_in,
    back_out,
    back,
    fold_out,
    fold_own,
    fold_in,
    cross_out,
    cross_in,
    branch_hidden,
    code_col,
    send_sem,
    recv_sem,
):
    ep, tp = lax.axis_index("ep"), lax.axis_index("tp")
    z, y, x, c = ep // 2, ep % 2, tp // 2, tp % 2
    token_count, quarter = tokens.shape
    ff = w_gate.shape[1]
    capacity = slots.shape[1]
    half = capacity // 2
    block = w_in.shape[0]

    def at(zz, yy, xx, cc):
        return (zz * 2 + yy, xx * 2 + cc)

    sibling = at(z, y, x, 1 - c)
    across = at(z, y, 1 - x, c)
    diagonal = at(z, y, 1 - x, 1 - c)
    pair = at(z, 1 - y, x, c)
    pair_user = at(z, 1 - y, x, y)
    pair_other = at(z, 1 - y, x, 1 - c)
    level = [z, z + 1 - 2 * (z % 2), (z + 2) % GROUPS, GROUPS - 1 - z]
    peer_of = [None] + [at(level[m], y, x, c) for m in range(1, GROUPS)]
    up = at((z + 1) % GROUPS, y, x, c)
    down = at((z + GROUPS - 1) % GROUPS, y, x, c)

    barrier = pltpu.get_barrier_semaphore()
    peers = [sibling, across, diagonal, pair, pair_other] + peer_of[1:]
    for peer in peers:
        pl.semaphore_signal(
            barrier, inc=1, device_id=peer, device_id_type=pl.DeviceIdType.MESH
        )

    branch_all[y, z, 0] = w_in[...]
    branch_all[y, z, 1] = w_out[...]
    floats = tokens[...].astype(F32)
    exact = floats * floats
    high = exact.astype(BF16)
    low = (exact - high.astype(F32)).astype(BF16)
    ones = jnp.ones((16, quarter), BF16)
    squares[0] = (dot_nt(ones, high) + dot_nt(ones, low))[:8]

    pl.semaphore_wait(barrier, len(peers))

    started = {}

    def send(number, source, target, device):
        copy = pltpu.make_async_remote_copy(
            src_ref=source,
            dst_ref=target,
            send_sem=send_sem.at[number],
            recv_sem=recv_sem.at[number],
            device_id=device,
            device_id_type=pl.DeviceIdType.MESH,
        )
        copy.start()
        started[number] = copy

    def arrived(number):
        started[number].wait_recv()

    send(6, squares.at[0], squares.at[1], sibling)
    send(7, squares.at[0], squares.at[2], across)
    send(8, squares.at[0], squares.at[3], diagonal)

    weights_of = ((w_gate, gate_all), (w_up, up_all), (w_down, down_all))

    def weight_copy(k, sem, device):
        source, target = weights_of[k]
        return pltpu.make_async_remote_copy(
            src_ref=source,
            dst_ref=target.at[c],
            send_sem=send_sem.at[2 * k + sem],
            recv_sem=recv_sem.at[2 * k + c],
            device_id=device,
            device_id_type=pl.DeviceIdType.MESH,
        )

    for k in range(3):
        weight_copy(k, 0, pair_user).start()

    @pl.when(c != y)
    def _():
        for k in range(3):
            weight_copy(k, 1, sibling).start()

    @pl.when(c == y)
    def _():
        for source, target in weights_of:
            target[c] = source[...]

    def weight_arrived(k):
        source, target = weights_of[k]

        def wait(h):
            pltpu.make_async_remote_copy(
                src_ref=source,
                dst_ref=target.at[h],
                send_sem=send_sem.at[2 * k],
                recv_sem=recv_sem.at[2 * k + h],
                device_id=sibling,
                device_id_type=pl.DeviceIdType.MESH,
            ).wait_recv()

        wait(1 - c)

        @pl.when(c != y)
        def _():
            wait(c)

    def relay(hop, upward):
        number = (12 if upward else 47) + hop - 1
        held = z - (hop - 1) if upward else z + (hop - 1)
        came = z - hop if upward else z + hop
        held, came = (held + GROUPS) % GROUPS, (came + GROUPS) % GROUPS
        sends = (z <= GROUPS - 2) & (z >= hop - 1)
        gets = z >= hop
        if not upward:
            sends = (z >= 1) & (z <= GROUPS - hop)
            gets = z <= GROUPS - 1 - hop

        def copy(row):
            return pltpu.make_async_remote_copy(
                src_ref=branch_all.at[y, row],
                dst_ref=branch_all.at[y, row],
                send_sem=send_sem.at[number],
                recv_sem=recv_sem.at[number],
                device_id=up if upward else down,
                device_id_type=pl.DeviceIdType.MESH,
            )

        return sends, gets, lambda: copy(held), lambda: copy(came)

    def relay_start(hop):
        for upward in (True, False):
            sends, _, outgoing, _ = relay(hop, upward)

            @pl.when(sends)
            def _():
                outgoing().start()

    def relay_arrived(hop):
        for upward in (True, False):
            _, gets, _, incoming = relay(hop, upward)

            @pl.when(gets)
            def _():
                incoming().wait_recv()

    def relay_sent(hop):
        for upward in (True, False):
            sends, _, outgoing, _ = relay(hop, upward)

            @pl.when(sends)
            def _():
                outgoing().wait_send()

    relay_start(1)
    ids = routing[0:1, :]
    group = lax.shift_right_logical(ids, 1)
    rows16 = lax.broadcasted_iota(jnp.int32, (16, token_count), 0)
    member = jnp.where(rows16 == group, 1.0, 0.0)
    earlier = jnp.where(
        lax.broadcasted_iota(jnp.int32, (token_count, token_count), 0)
        < lax.broadcasted_iota(jnp.int32, (token_count, token_count), 1),
        1.0,
        0.0,
    ).astype(BF16)
    before = dot(member.astype(BF16), earlier)
    place = jnp.sum(member * before, axis=0, keepdims=True)
    code = group.astype(F32) * capacity + place
    code_col[...] = jnp.transpose(jnp.broadcast_to(code, (8, token_count)))
    first, second = route_weight[0:1, :], route_weight[1:2, :]
    even_first = (ids & 1) == 0
    for_even = jnp.where(even_first, first, second)
    for_odd = jnp.where(even_first, second, first)
    weights = jnp.where((rows16 & 1) == 0, for_even, for_odd)
    weights_high = weights.astype(BF16)
    weights_low = (weights - weights_high.astype(F32)).astype(BF16)

    for number in (6, 7, 8):
        arrived(number)
    total = squares[0] + squares[1] + squares[2] + squares[3]
    factor = lax.rsqrt(total / (4 * quarter) + epsilon)
    factor_col = jnp.transpose(factor)[:, 0:1]
    normed[0] = (tokens[...].astype(F32) * factor_col * gain[...]).astype(BF16)
    send(10, normed.at[0], normed.at[2], across)
    send(9, normed.at[0], normed.at[1], sibling)

    def dispatch(s):
        send(19 + s, slots_out.at[s], slots.at[s], peer_of[s])
        send(22 + s, scale_out.at[s], scale.at[s], peer_of[s])

    slot_row = lax.broadcasted_iota(jnp.int32, (capacity, token_count), 0)
    for s in (2, 3, 1, 0):
        wanted = (slot_row + level[s] * capacity).astype(F32)
        choose = jnp.where(wanted == code, 1.0, 0.0).astype(BF16)
        rows = dot(choose, normed[0]).astype(BF16)
        slot_weights = (dot_nt(weights_high, choose) + dot_nt(weights_low, choose))[:8]
        if s == 0:
            slots[0] = rows
            scale[0] = slot_weights
            send(26, slots.at[0], slots_s.at[0], sibling)
        else:
            slots_out[s] = rows
            scale_out[s] = slot_weights
            if s > 1:
                dispatch(s)

    def project(s, start, weights):
        own = slots[s, pl.ds(start, half), :]
        other = slots_s[s, pl.ds(start, half), :]
        return dot(own, weights[c]) + dot(other, weights[1 - c])

    mine = pl.multiple_of(x * half, half)
    theirs = pl.multiple_of((1 - x) * half, half)

    def forward(s):
        if s:
            arrived(19 + s)
            send(26 + s, slots.at[s], slots_s.at[s], sibling)

    sides = (slice(0, ff), slice(ff, 2 * ff))

    def stage_a(s):
        arrived(26 + s)
        for side, weights in zip(sides, (gate_all, up_all)):
            part_out[s, :, side] = project(s, theirs, weights).astype(BF16)
        send(30 + s, part_out.at[s], part_in.at[s], across)
        for side, weights in zip(sides, (gate_all, up_all)):
            part_own[s, :, side] = project(s, mine, weights)

    def stage_a_own(k):
        side, weights = sides[k], (gate_all, up_all)[k]
        part_out[0, :, side] = project(0, theirs, weights).astype(BF16)
        send(30 + 20 * k, part_out.at[0, :, side], part_in.at[0, :, side], across)
        part_own[0, :, side] = project(0, mine, weights)

    def stage_b(s):
        arrived(30 + s)
        if s == 0:
            arrived(50)
        gate_sum = part_own[s, :, :ff] + part_in[s, :, :ff].astype(F32)
        up_sum = part_own[s, :, ff:] + part_in[s, :, ff:].astype(F32)
        hidden[s, pl.ds(mine, half), :] = (silu(gate_sum) * up_sum).astype(BF16)
        kept = hidden.at[s, pl.ds(mine, half), :]
        send(34 + s, kept, kept, across)

    def stage_c(s):
        arrived(34 + s)
        if s:
            arrived(22 + s)
        columns = jnp.transpose(scale[s])
        weight = jnp.where(c == 0, columns[:, 0:1], columns[:, 1:2])
        units = hidden[s]
        half_out[s] = (dot(units, down_all[1 - c]) * weight).astype(BF16)
        send(38 + s, half_out.at[s], half_in.at[s], sibling)
        half_own[s] = dot(units, down_all[c]) * weight

    def stage_d(s):
        arrived(38 + s)
        both = (half_own[s] + half_in[s].astype(F32)).astype(BF16)
        if s == 0:
            back[0] = both
        else:
            back_out[s] = both
            send(41 + s, back_out.at[s], back.at[s], peer_of[s])

    def pair_send(m):
        rows = branch_all.at[y, level[m]]
        send(15 + m, rows, rows, pair)

    weight_arrived(0)
    arrived(26)
    stage_a_own(0)
    weight_arrived(1)
    stage_a_own(1)
    dispatch(1)
    relay_arrived(1)
    relay_start(2)
    pair_send(0)
    pair_send(1)
    forward(2)
    stage_a(2)
    arrived(10)
    send(11, normed.at[2], normed.at[3], sibling)
    stage_b(0)
    forward(3)
    stage_a(3)
    relay_arrived(2)
    relay_start(3)
    pair_send(2)
    stage_b(2)
    stage_b(3)
    relay_arrived(3)
    pair_send(3)
    weight_arrived(2)
    stage_c(2)
    forward(1)
    stage_a(1)
    stage_d(2)
    stage_c(3)
    stage_c(0)
    stage_d(3)
    stage_d(0)

    arrived(9)
    arrived(11)
    for m in range(GROUPS):
        arrived(15 + m)
    quarters = (tp, x * 2 + 1 - c, (1 - x) * 2 + c, (1 - x) * 2 + 1 - c)
    sums = jnp.zeros((token_count, block), F32)
    for k, q in enumerate(quarters):
        sums = sums + dot(normed[k, :, :block], branch_all[0, q, 0])
        sums = sums + dot(normed[k, :, block:], branch_all[1, q, 0])
    branch_hidden[...] = silu(sums).astype(BF16)

    def branch_part(q, side):
        return dot(branch_hidden[...], branch_all[side, q, 1])

    for side in range(2):
        columns = slice(side * block, (side + 1) * block)
        fold_out[0, :, columns] = branch_part(quarters[1], side).astype(BF16)
        fold_out[1, :, columns] = branch_part(quarters[3], side).astype(BF16)
    send(45, fold_out, fold_in, sibling)

    stage_b(1)

    arrived(45)
    for side in range(2):
        columns = slice(side * block, (side + 1) * block)
        cross_out[:, columns] = (
            branch_part(quarters[2], side) + fold_in[1, :, columns].astype(F32)
        ).astype(BF16)
    send(46, cross_out, cross_in, across)
    stage_c(1)
    stage_d(1)
    for side in range(2):
        columns = slice(side * block, (side + 1) * block)
        fold_own[:, columns] = branch_part(quarters[0], side) + fold_in[0, :, columns].astype(F32)

    slot_lane = lax.broadcasted_iota(jnp.int32, (token_count, capacity), 1)

    def restore(s):
        wanted = (slot_lane + level[s] * capacity).astype(F32)
        choose = jnp.where(wanted == code_col[:, 0:1], 1.0, 0.0).astype(BF16)
        return dot(choose, back[s])

    half_own_sum = restore(0)
    for s in (2, 3, 1):
        arrived(41 + s)
        half_own_sum = half_own_sum + restore(s)
    arrived(46)
    branch = fold_own[...] + cross_in[...].astype(F32)
    gate = 1.0 / (1.0 + jnp.exp(-branch_gate[...]))
    out[...] = (half_own_sum + gate * branch).astype(BF16)
    for copy in started.values():
        copy.wait_send()
    for hop in range(1, GROUPS):
        relay_sent(hop)
    for k in range(3):
        weight_copy(k, 0, pair_user).wait_send()

    @pl.when(c != y)
    def _():
        for k in range(3):
            weight_copy(k, 1, sibling).wait_send()


def pair_body(
    tokens,
    norm_gain,
    routing,
    route_weight,
    w_gate,
    w_up,
    w_down,
    w_branch_in,
    w_branch_out,
    branch_gate,
):
    count, quarter = tokens.shape
    ff = w_gate.shape[2]
    block = w_branch_in.shape[0]
    cap = count // 2
    half = cap // 2
    vmem = pltpu.VMEM
    rows = (GROUPS, cap, quarter)
    scratch = [
        vmem((2, quarter, ff), BF16),
        vmem((2, quarter, ff), BF16),
        vmem((2, ff, quarter), BF16),
        vmem((4, 8, count), F32),
        vmem((4, count, quarter), BF16),
        vmem((2, GROUPS, 2, block, block), BF16),
        vmem(rows, BF16),
        vmem(rows, BF16),
        vmem(rows, BF16),
        vmem((GROUPS, 8, cap), F32),
        vmem((GROUPS, 8, cap), F32),
        vmem((GROUPS, half, 2 * ff), BF16),
        vmem((GROUPS, half, 2 * ff), F32),
        vmem((GROUPS, half, 2 * ff), BF16),
        vmem((GROUPS, cap, ff), BF16),
        vmem(rows, BF16),
        vmem(rows, F32),
        vmem(rows, BF16),
        vmem(rows, BF16),
        vmem(rows, BF16),
        vmem((2, count, quarter), BF16),
        vmem((count, quarter), F32),
        vmem((2, count, quarter), BF16),
        vmem((count, quarter), BF16),
        vmem((count, quarter), BF16),
        vmem((count, block), BF16),
        vmem((count, 8), F32),
        pltpu.SemaphoreType.DMA((COPIES,)),
        pltpu.SemaphoreType.DMA((COPIES,)),
    ]
    return pl.pallas_call(
        pair_kernel,
        out_shape=jax.ShapeDtypeStruct((count, quarter), BF16),
        in_specs=[pl.BlockSpec(memory_space=vmem)] * 10,
        out_specs=pl.BlockSpec(memory_space=vmem),
        scratch_shapes=scratch,
        compiler_params=pltpu.CompilerParams(
            collective_id=0, has_side_effects=True, vmem_limit_bytes=60 * 1024 * 1024
        ),
    )(
        tokens,
        norm_gain[None, :],
        routing.T,
        route_weight.T,
        w_gate[0],
        w_up[0],
        w_down[0],
        w_branch_in,
        w_branch_out,
        branch_gate[None, :],
    )


def solution(mesh):
    return jax.shard_map(
        pair_body if mesh.shape["ep"] == 2 * GROUPS and mesh.shape["tp"] == 4 else body,
        mesh=mesh,
        in_specs=(
            P("ep", "tp"),
            P("tp"),
            P("ep", None),
            P("ep", None),
            P("ep", "tp", None),
            P("ep", "tp", None),
            P("ep", None, "tp"),
            P("ep", "tp"),
            P("tp", "ep"),
            P("tp"),
        ),
        out_specs=P("ep", "tp"),
        check_vma=False,
    )
```
